512 devices in a mesh: grp: 2 (over y), dp: 8 (over x), kv: 16 (over z), tp: 2 (over core).
Axes of the slice: x: 8, y: 2, z: 16, core: 2. Of those that a mesh axis runs over, the one named last changes fastest.
The devices are a block of a 8x8x16 slice.
Arguments:
- inputs: bfloat16 [512, 4096], P(('grp', 'dp'), 'kv'), parts along dimension 0, may hold values from -6 to 6
- gain_in: float32 [4096], P('kv'), may hold values from 0.1 to 1.9
- w_gate: bfloat16 [4096, 2048], P('kv', 'tp'), may hold values from -0.09375 to 0.09375
- w_input: bfloat16 [4096, 2048], P('kv', 'tp'), may hold values from -0.09375 to 0.09375
- w_bproj: bfloat16 [4096, 1024], P('kv', 'tp'), may hold values from -0.09375 to 0.09375
- w_cproj: bfloat16 [4096, 1024], P('kv', 'tp'), may hold values from -0.09375 to 0.09375
- w_step: bfloat16 [4096, 32], P('kv', 'tp'), may hold values from -0.09375 to 0.09375
- conv_input: float32 [4, 2048], P(None, 'tp'), may hold values from -3 to 3
- conv_bproj: float32 [4, 1024], P(None, 'tp'), may hold values from -3 to 3
- conv_cproj: float32 [4, 1024], P(None, 'tp'), may hold values from -3 to 3
- tail_input: bfloat16 [512, 3, 2048], P(('grp', 'dp', 'kv'), None, 'tp'), parts along dimension 0, may hold values from -6 to 6
- tail_bproj: bfloat16 [512, 3, 1024], P(('grp', 'dp', 'kv'), None, 'tp'), parts along dimension 0, may hold values from -6 to 6
- tail_cproj: bfloat16 [512, 3, 1024], P(('grp', 'dp', 'kv'), None, 'tp'), parts along dimension 0, may hold values from -6 to 6
- step_bias: float32 [32], P('tp'), may hold values from -3 to 0
- decay_log: float32 [32], P('tp'), may hold values from -2 to 2
- block_input: bfloat16 [512, 128, 2048], P(('grp', 'dp', 'kv'), None, 'tp'), parts along dimension 0, may hold values from -6 to 6
- block_bproj: bfloat16 [512, 128, 1024], P(('grp', 'dp', 'kv'), None, 'tp'), parts along dimension 0, may hold values from -0.59765625 to 0.59765625
- block_step: float32 [512, 128, 32], P(('grp', 'dp', 'kv'), None, 'tp'), parts along dimension 0, may hold values from 0.005 to 0.2
- lengths: int32 [512], P(('grp', 'dp', 'kv')), parts along dimension 0, may hold values from 1 to 127, 8192 in all
- state: float32 [512, 32, 64, 128], P(('grp', 'dp', 'kv'), 'tp'), parts along dimension 0, may hold values from -0.6 to 0.6
- gain_mix: float32 [2048], P('tp'), may hold values from 0.1 to 1.9
- w_out: bfloat16 [2048, 4096], P('tp', 'kv'), may hold values from -0.125 to 0.125
- gain_mlp: float32 [4096], P(('kv', 'tp')), may hold values from 0.1 to 1.9
- w_up: bfloat16 [4096, 16384], P(('kv', 'tp'), 'dp'), may hold values from -0.09375 to 0.09375
- w_down: bfloat16 [16384, 4096], P('dp', ('kv', 'tp')), may hold values from -0.046875 to 0.046875
Outputs:
- layer_out: bfloat16 [512, 4096], P(('grp', 'dp'), ('kv', 'tp')), parts along dimension 0
The draws below stay inside these ranges and needn't reach their ends.
There are 2 independent parts, one for each index of `grp`. The reference program is written for one: setup_inputs(seed, part) draws one part's arguments, and reference() takes and returns one part's arrays. A program takes and returns all parts, laid end to end along the dimension named above; an argument that names none is the same for every part. Nothing has to cross between parts.
Inputs may be any that keep to these rules, and one draw needn't show every extreme that they name: `lengths`: the number of live positions before the new token in each sequence's current block; the largest equals 127 in every draw.
All inputs are finite; a program needn't handle non-finite values.
Results may differ from the reference program's by a relative error of at most 0.012.
Values may be sent and summed in bfloat16 or wider, within the bound.
No kernel may reach another device: no remote copies, remote signals or barrier semaphores. Data moves between devices by JAX's collectives and lax.ppermute only.
A program may use at most 64 MiB of HBM per device.

```python
import math
import jax
import jax.numpy as jnp
import numpy as np
from jax import lax

D = 4096
SSM_HEADS = 32
HEAD_DIM = 64
GROUPS = 8
D_STATE = 128
FF = 16384
TAPS = 4
BLK = 128
SSM_WIDTH = 2048
SEQS = 256


def steps_of(stream_key, dims, cuts, smallest, high):
    loudness, own = 1.0, jax.random.fold_in(stream_key, 6)
    for dim, parts in cuts:
        steps = jnp.exp(jax.random.uniform(jax.random.fold_in(own, dim), (parts,), jnp.float32, smallest / len(cuts), high / len(cuts)))
        loudness = loudness * jnp.repeat(steps, dims[dim] // parts).reshape([-1 if axis == dim else 1 for axis in range(len(dims))])
    return loudness


def split_up(number_of, total, bound, lean):
    loads = [(1 << 20) // math.isqrt(rank ** lean) + 1 for rank in range(2, number_of + 1)]
    surplus, given = total - bound - (number_of - 1), [1] * (number_of - 1)
    while surplus > 0:
        free = [i for i in range(number_of - 1) if given[i] < bound]
        mass, left = sum([loads[i] for i in free]), surplus
        for i in free:
            more = min(bound - given[i], max(1, left * loads[i] // mass), surplus)
            given[i] = given[i] + more
            surplus = surplus - more
    return np.array([bound] + given)


def uneven_parts(key, count, total, limit, slope):
    if count == 2:
        one = jax.random.randint(key, (), max(1, total - limit), min(limit, total - 1) + 1)
        return jnp.stack([one, total - one])
    sizes = jnp.asarray(split_up(count, total, limit, slope), jnp.int32)
    twos = (count - 1) // 2
    giver, taker = sizes[1:1 + 2 * twos:2], sizes[2:2 + 2 * twos:2]
    room = jnp.minimum(giver - 1, limit - taker)
    shifted = jax.random.randint(jax.random.fold_in(key, 1), (twos,), 0, 1 << 20) % (room + 1)
    sizes = sizes.at[1:1 + 2 * twos:2].set(giver - shifted).at[2:2 + 2 * twos:2].set(taker + shifted)
    return sizes[jax.random.permutation(jax.random.fold_in(key, 2), count)]


def centred(rng, extent, scale, limit, split=(), held_as=jnp.bfloat16):
    factor_of = steps_of(rng, extent, split, -0.22, 0.18) if split else 1.0
    array = jax.random.normal(rng, extent, jnp.float32) * scale * factor_of
    return jnp.minimum(jnp.maximum(array, -limit), limit).astype(held_as)


def setup_inputs(seed: int = 0, part: int = 0) -> dict:
    seeds = jax.random.split(jax.random.key(seed), 26)
    part_keys = jax.random.split(jax.random.fold_in(seeds[25], part), 26)
    inputs = centred(part_keys[0], (SEQS, D), 1.0, 6.0, ((0, 8), (1, 16)))
    gain_in = jnp.clip(1.0 + 0.18 * jax.random.normal(seeds[1], (D,), jnp.float32), 0.1, 1.9)
    w_gate = centred(seeds[2], (D, SSM_WIDTH), D ** -0.5, 0.09375, ((0, 16), (1, 2)))
    w_input = centred(seeds[3], (D, SSM_WIDTH), D ** -0.5, 0.09375, ((0, 16), (1, 2)))
    w_bproj = centred(seeds[4], (D, GROUPS * D_STATE), D ** -0.5, 0.09375, ((0, 16), (1, 2)))
    w_cproj = centred(seeds[5], (D, GROUPS * D_STATE), D ** -0.5, 0.09375, ((0, 16), (1, 2)))
    w_step = centred(seeds[6], (D, SSM_HEADS), D ** -0.5, 0.09375, ((0, 16), (1, 2)))
    conv_input = centred(seeds[7], (TAPS, SSM_WIDTH), TAPS ** -0.5, 3.0, ((1, 2),), jnp.float32)
    conv_bproj = centred(seeds[8], (TAPS, GROUPS * D_STATE), TAPS ** -0.5, 3.0, ((1, 2),), jnp.float32)
    conv_cproj = centred(seeds[9], (TAPS, GROUPS * D_STATE), TAPS ** -0.5, 3.0, ((1, 2),), jnp.float32)
    tail_input = centred(part_keys[10], (SEQS, TAPS - 1, SSM_WIDTH), 1.0, 6.0, ((0, 128), (2, 2)))
    tail_bproj = centred(part_keys[11], (SEQS, TAPS - 1, GROUPS * D_STATE), 1.0, 6.0, ((0, 128), (2, 2)))
    tail_cproj = centred(part_keys[12], (SEQS, TAPS - 1, GROUPS * D_STATE), 1.0, 6.0, ((0, 128), (2, 2)))
    step_bias = jnp.clip(-3.0 + 3.0 * jax.random.uniform(seeds[13], (SSM_HEADS,), jnp.float32) ** steps_of(seeds[13], (SSM_HEADS,), ((0, 2),), -0.2, 0.2), -3.0, 0.0)
    decay_log = jnp.clip(jax.random.uniform(seeds[14], (SSM_HEADS,), jnp.float32, -2.0, 2.0) * steps_of(seeds[14], (SSM_HEADS,), ((0, 2),), -0.4, 0.0), -2.0, 2.0)
    block_input = centred(part_keys[15], (SEQS, BLK, SSM_WIDTH), 1.0, 6.0, ((0, 128), (2, 2)))
    block_bproj = centred(part_keys[16], (SEQS, BLK, GROUPS * D_STATE), 0.1, 0.59765625, ((0, 128), (2, 2)))
    block_step = jnp.clip(jnp.exp(math.log(0.2) - 3.6888795 * jax.random.uniform(part_keys[17], (SEQS, BLK, SSM_HEADS), jnp.float32) ** steps_of(part_keys[17], (SEQS, BLK, SSM_HEADS), ((0, 128), (2, 2)), -0.2, 0.2)), 0.005, 0.2)
    lengths = uneven_parts(part_keys[18], SEQS, SEQS * BLK // 4, BLK - 1, 2).astype(jnp.int32)
    state = centred(part_keys[19], (SEQS, SSM_HEADS, HEAD_DIM, D_STATE), 0.1, 0.6, ((0, 128), (1, 2)), jnp.float32)
    gain_mix = jnp.clip(1.0 + 0.18 * jax.random.normal(seeds[20], (SSM_WIDTH,), jnp.float32), 0.1, 1.9)
    w_out = centred(seeds[21], (SSM_WIDTH, D), SSM_WIDTH ** -0.5, 0.125, ((0, 2), (1, 16)))
    gain_mlp = jnp.clip(1.0 + 0.18 * jax.random.normal(seeds[22], (D,), jnp.float32), 0.1, 1.9)
    w_up = centred(seeds[23], (D, FF), D ** -0.5, 0.09375, ((0, 32), (1, 8)))
    w_down = centred(seeds[24], (FF, D), FF ** -0.5, 0.046875, ((0, 8), (1, 32)))
    return {"inputs": inputs, "gain_in": gain_in, "w_gate": w_gate, "w_input": w_input, "w_bproj": w_bproj, "w_cproj": w_cproj, "w_step": w_step, "conv_input": conv_input, "conv_bproj": conv_bproj, "conv_cproj": conv_cproj, "tail_input": tail_input, "tail_bproj": tail_bproj, "tail_cproj": tail_cproj, "step_bias": step_bias, "decay_log": decay_log, "block_input": block_input, "block_bproj": block_bproj, "block_step": block_step, "lengths": lengths, "state": state, "gain_mix": gain_mix, "w_out": w_out, "gain_mlp": gain_mlp, "w_up": w_up, "w_down": w_down}


EPS = 1e-06

def convolve(history, weights, newest):
    summed = weights[TAPS - 1].astype(jnp.float32) * newest
    for offset in range(TAPS - 1):
        summed = summed + weights[offset].astype(jnp.float32) * history[:, offset].astype(jnp.float32)
    return jax.nn.silu(summed)

def reference(inputs, gain_in, w_gate, w_input, w_bproj, w_cproj, w_step, conv_input, conv_bproj, conv_cproj, tail_input, tail_bproj, tail_cproj, step_bias, decay_log, block_input, block_bproj, block_step, lengths, state, gain_mix, w_out, gain_mlp, w_up, w_down):
    stream = inputs.astype(jnp.float32)
    inverse = lax.rsqrt(lax.optimization_barrier(jnp.mean(stream * stream, axis=1, keepdims=True)) + EPS)
    scaled = (stream * gain_in.astype(jnp.float32)).astype(jnp.bfloat16)
    gate_pre = jnp.dot(scaled, w_gate, preferred_element_type=jnp.float32) * inverse
    value_pre = jnp.dot(scaled, w_input, preferred_element_type=jnp.float32) * inverse
    b_pre = jnp.dot(scaled, w_bproj, preferred_element_type=jnp.float32) * inverse
    c_pre = jnp.dot(scaled, w_cproj, preferred_element_type=jnp.float32) * inverse
    step_pre = jnp.dot(scaled, w_step, preferred_element_type=jnp.float32) * inverse
    current = convolve(tail_input, conv_input, value_pre)
    b_now = convolve(tail_bproj, conv_bproj, b_pre)
    c_now = convolve(tail_cproj, conv_cproj, c_pre)
    step_size = jax.nn.softplus(step_pre + step_bias.astype(jnp.float32))
    decay_rate = -jnp.exp(decay_log.astype(jnp.float32))
    positions = jnp.arange(BLK, dtype=jnp.int32)
    live_rows = (positions[None, :] < lengths[:, None].astype(jnp.int32)).astype(jnp.float32)
    block_steps = block_step.astype(jnp.float32)
    masked = block_steps * live_rows[:, :, None]
    later_steps = lax.optimization_barrier(jnp.sum(masked, axis=1, keepdims=True)) - jnp.cumsum(masked, axis=1)
    decays = jnp.exp(decay_rate * (step_size[:, None, :] + later_steps)) * live_rows[:, :, None]
    per_group = SSM_HEADS // GROUPS
    c_query = lax.optimization_barrier(c_now.astype(jnp.bfloat16)).astype(jnp.float32).reshape(SEQS, GROUPS, D_STATE)
    keys = block_bproj.astype(jnp.float32).reshape(SEQS, BLK, GROUPS, D_STATE)
    scores = jnp.repeat(jnp.einsum('bsgn,bgn->bsg', keys, c_query), per_group, axis=2)
    weights = lax.optimization_barrier((decays * scores * block_steps).astype(jnp.bfloat16)).astype(jnp.float32)
    values = block_input.astype(jnp.float32).reshape(SEQS, BLK, SSM_HEADS, HEAD_DIM)
    inner_sum = jnp.einsum('bsh,bshp->bhp', weights, values)
    c_full = c_now.reshape(SEQS, GROUPS, D_STATE)
    b_full = b_now.reshape(SEQS, GROUPS, D_STATE)
    own_score = jnp.repeat(lax.optimization_barrier(jnp.sum(c_full * b_full, axis=2)), per_group, axis=1)
    own_term = (step_size * own_score)[:, :, None] * current.reshape(SEQS, SSM_HEADS, HEAD_DIM)
    carried = jnp.exp(decay_rate * (step_size + lax.optimization_barrier(jnp.sum(masked, axis=1))))
    c_heads = jnp.repeat(c_full, per_group, axis=1)
    readout = jnp.einsum('bhpn,bhn->bhp', state.astype(jnp.float32), c_heads, precision=lax.Precision.HIGHEST)
    mixed = (inner_sum + own_term + carried[:, :, None] * readout).reshape(SEQS, SSM_WIDTH) * jax.nn.silu(gate_pre)
    inverse_mix = lax.rsqrt(lax.optimization_barrier(jnp.mean(mixed * mixed, axis=1, keepdims=True)) + EPS)
    normed = (mixed * inverse_mix * gain_mix.astype(jnp.float32)).astype(jnp.bfloat16)
    hidden = (stream + jnp.dot(normed, w_out, preferred_element_type=jnp.float32)).astype(jnp.bfloat16)
    hidden_f = hidden.astype(jnp.float32)
    inverse_mlp = lax.rsqrt(lax.optimization_barrier(jnp.mean(hidden_f * hidden_f, axis=1, keepdims=True)) + EPS)
    lifted = (hidden_f * gain_mlp.astype(jnp.float32)).astype(jnp.bfloat16)
    raised = jnp.dot(lifted, w_up, preferred_element_type=jnp.float32) * inverse_mlp
    hidden_units = jnp.square(jax.nn.relu(raised)).astype(jnp.bfloat16)
    return (hidden_f + jnp.dot(hidden_units, w_down, preferred_element_type=jnp.float32)).astype(jnp.bfloat16)
```

```python
import jax
import jax.numpy as jnp
from jax import lax
from jax.sharding import PartitionSpec as P

D = 4096
HEAD_DIM = 64
D_STATE = 128
TAPS = 4
SSM_WIDTH = 2048
LANES = 128

EPS = 1e-06
BF16 = jnp.bfloat16
F32 = jnp.float32


def two_words(x):
    high = lax.reduce_precision(x, 8, 7)
    return high.astype(BF16), (x - high).astype(BF16)


def to_everyone(shard, axes):
    size = lax.axis_size(axes)
    return lax.all_to_all(
        jnp.broadcast_to(shard[None], (size, *shard.shape)), axes, 0, 0, tiled=True
    )


def from_partner(x):
    size = lax.axis_size("tp")
    return lax.ppermute(x, "tp", [(i, (i + 1) % size) for i in range(size)])


def exchanged(weight, dim, core):
    half = weight.shape[dim] // 2
    mine = lax.dynamic_slice_in_dim(weight, core * half, half, dim)
    other = lax.dynamic_slice_in_dim(weight, (1 - core) * half, half, dim)
    return mine, from_partner(other)


def in_core_order(mine, other, core, dim):
    return jnp.where(
        core == 0,
        jnp.concatenate([mine, other], axis=dim),
        jnp.concatenate([other, mine], axis=dim),
    )


def convolve(history, weights, newest):
    summed = weights[TAPS - 1] * newest
    for offset in range(TAPS - 1):
        summed = summed + weights[offset] * history[:, offset].astype(F32)
    return jax.nn.silu(summed)


def per_device(
    inputs,
    gain_in,
    w_gate,
    w_input,
    w_bproj,
    w_cproj,
    w_step,
    conv_input,
    conv_bproj,
    conv_cproj,
    tail_input,
    tail_bproj,
    tail_cproj,
    step_bias,
    decay_log,
    block_input,
    block_bproj,
    block_step,
    lengths,
    state,
    gain_mix,
    w_out,
    gain_mlp,
    w_up,
    w_down,
):
    core = lax.axis_index("tp")
    n_kv, n_dp, n_tp = lax.axis_size("kv"), lax.axis_size("dp"), lax.axis_size("tp")
    stream = inputs.astype(F32)
    rows = inputs.shape[0]
    squares = jnp.sum(stream * stream, axis=1)
    scaled = (stream * gain_in).astype(BF16)
    matrices = (w_gate, w_input, w_bproj, w_cproj)
    pieces = [jnp.dot(scaled, weight, preferred_element_type=F32).astype(BF16) for weight in matrices]
    pieces += two_words(jnp.dot(scaled, w_step, preferred_element_type=F32))
    pieces += two_words(squares[:, None])
    bounds = [0]
    for piece in pieces:
        bounds.append(bounds[-1] + piece.shape[1])
    spare = -bounds[-1] % LANES
    pieces.append(jnp.zeros((rows, spare), BF16))
    sent = jnp.concatenate(pieces, axis=1).reshape(n_kv, rows // n_kv, -1)
    arrived = lax.all_to_all(sent, "kv", 0, 0, tiled=True)
    projected = jnp.sum(arrived.astype(F32), axis=0)

    out_mine, out_other = exchanged(w_out, 1, core)
    up_mine, up_other = exchanged(w_up, 1, core)
    down_mine, down_other = exchanged(w_down, 0, core)
    gain_other = from_partner(gain_mlp)
    out_weight = jnp.concatenate([out_mine, out_other], axis=0)
    up_weight = jnp.concatenate([up_mine, up_other], axis=0)
    down_weight = in_core_order(down_mine, down_other, core, 1)
    up_gain = jnp.concatenate([gain_mlp, gain_other])

    parts = [projected[:, a:b] for a, b in zip(bounds[:-1], bounds[1:])]
    inverse = lax.rsqrt((parts[6] + parts[7]) / D + EPS)
    gate_pre, value_pre, b_pre, c_pre = [parts[k] * inverse for k in range(4)]
    step_pre = (parts[4] + parts[5]) * inverse
    seq_count = lengths.shape[0]
    head_count = step_bias.shape[0]
    group_count = w_bproj.shape[1] // D_STATE
    block_len = block_step.shape[1]
    per_group = head_count // group_count
    current = convolve(tail_input, conv_input, value_pre)
    b_now = convolve(tail_bproj, conv_bproj, b_pre)
    c_now = convolve(tail_cproj, conv_cproj, c_pre)
    step_size = jax.nn.softplus(step_pre + step_bias)
    decay_rate = -jnp.exp(decay_log)
    positions = lax.broadcasted_iota(jnp.int32, (1, block_len), 1)
    live_rows = (positions < lengths[:, None]).astype(F32)
    masked = block_step * live_rows[:, :, None]
    later_steps = jnp.sum(masked, axis=1, keepdims=True) - jnp.cumsum(masked, axis=1)
    decays = jnp.exp(decay_rate * (step_size[:, None, :] + later_steps)) * live_rows[:, :, None]
    c_query = c_now.astype(BF16).reshape(seq_count, group_count, D_STATE)
    keys = block_bproj.reshape(seq_count, block_len, group_count, D_STATE)
    scores = jnp.einsum("bsgn,bgn->bsg", keys, c_query, preferred_element_type=F32)
    scores = jnp.repeat(scores, per_group, axis=2)
    weights = (decays * scores * block_step).astype(BF16)
    values = block_input.reshape(seq_count, block_len, head_count, HEAD_DIM)
    inner_sum = jnp.einsum("bsh,bshp->bhp", weights, values, preferred_element_type=F32)
    c_full = c_now.reshape(seq_count, group_count, D_STATE)
    b_full = b_now.reshape(seq_count, group_count, D_STATE)
    own_score = jnp.repeat(jnp.sum(c_full * b_full, axis=2), per_group, axis=1)
    own_term = (step_size * own_score)[:, :, None] * current.reshape(
        seq_count, head_count, HEAD_DIM
    )
    carried = jnp.exp(decay_rate * (step_size + jnp.sum(masked, axis=1)))
    c_heads = jnp.repeat(c_full, per_group, axis=1)
    readout = jnp.einsum("bhpn,bhn->bhp", state, c_heads, precision=lax.Precision.HIGHEST)
    mixed = (inner_sum + own_term + carried[:, :, None] * readout).reshape(
        seq_count, -1
    ) * jax.nn.silu(gate_pre)

    width = mixed.shape[1]
    local_sq = two_words(jnp.sum(mixed * mixed, axis=1, keepdims=True))
    row = jnp.concatenate(
        [(mixed * gain_mix).astype(BF16), *local_sq, jnp.zeros((seq_count, LANES - 2), BF16)], axis=1
    )
    whole = to_everyone(row, ("kv", "tp")).reshape(n_kv, n_tp, seq_count, -1)
    whole = jnp.moveaxis(whole, 1, 0).reshape(n_tp, rows, -1)
    total_sq = jnp.sum(whole[:, :, width : width + 2].astype(F32), axis=(0, 2))
    halves = whole[:, :, :width]
    channels = jnp.concatenate(
        [
            lax.dynamic_index_in_dim(halves, core, 0, keepdims=False),
            lax.dynamic_index_in_dim(halves, 1 - core, 0, keepdims=False),
        ],
        axis=1,
    )
    mixed_in = jnp.dot(channels, out_weight, preferred_element_type=F32)
    mixed_in = mixed_in * lax.rsqrt(total_sq / SSM_WIDTH + EPS)[:, None]
    column_count = mixed_in.shape[1]
    residual = lax.dynamic_slice_in_dim(stream, core * column_count, column_count, 1)
    hidden = (residual + mixed_in).astype(BF16)

    all_hidden = to_everyone(hidden, ("dp", "tp")).reshape(n_dp, n_tp, rows, -1)
    all_hidden = jnp.moveaxis(all_hidden, 1, 0).reshape(n_tp, n_dp * rows, -1)
    all_hidden = jnp.concatenate(
        [
            lax.dynamic_index_in_dim(all_hidden, core, 0, keepdims=False),
            lax.dynamic_index_in_dim(all_hidden, 1 - core, 0, keepdims=False),
        ],
        axis=1,
    ).astype(F32)
    row_sq = jnp.sum(all_hidden * all_hidden, axis=1)
    lifted = (all_hidden * up_gain).astype(BF16)
    raised = lax.dot_general(
        up_weight, lifted, (((0,), (1,)), ((), ())), preferred_element_type=F32
    ).astype(BF16)
    seqs = raised.shape[1]
    extra = jnp.concatenate(
        [*[w[None] for w in two_words(row_sq)], jnp.zeros((6, seqs), BF16)], axis=0
    )
    sent = jnp.concatenate(
        [
            raised.reshape(n_kv, -1, seqs),
            jnp.broadcast_to(extra[None], (n_kv, *extra.shape)),
        ],
        axis=1,
    )
    arrived = lax.all_to_all(sent, "kv", 0, 0, tiled=True)
    shares = jnp.sum(arrived.astype(F32), axis=0)
    unit_count = shares.shape[0] - 8
    sq_sum = shares[unit_count] + shares[unit_count + 1]
    units = jnp.square(
        jax.nn.relu(shares[:unit_count] * lax.rsqrt(sq_sum / D + EPS)[None, :])
    ).astype(BF16)
    hidden_units = lax.all_gather(units, "kv", axis=0, tiled=True)
    lowered = lax.dot_general(
        hidden_units, down_weight, (((0,), (0,)), ((), ())), preferred_element_type=F32
    ).astype(BF16)
    lowered = lowered.reshape(n_dp, rows, n_tp, -1)
    lowered = jnp.moveaxis(lowered, 2, 1).reshape(n_dp * n_tp, rows, -1)
    lowered = lax.all_to_all(lowered, ("dp", "tp"), 0, 0, tiled=True)
    return (hidden.astype(F32) + jnp.sum(lowered.astype(F32), axis=0)).astype(BF16)


def solution(mesh):
    return jax.shard_map(
        per_device,
        mesh=mesh,
        in_specs=(
            P(("grp", "dp"), "kv"),
            P("kv"),
            P("kv", "tp"),
            P("kv", "tp"),
            P("kv", "tp"),
            P("kv", "tp"),
            P("kv", "tp"),
            P(None, "tp"),
            P(None, "tp"),
            P(None, "tp"),
            P(("grp", "dp", "kv"), None, "tp"),
            P(("grp", "dp", "kv"), None, "tp"),
            P(("grp", "dp", "kv"), None, "tp"),
            P("tp"),
            P("tp"),
            P(("grp", "dp", "kv"), None, "tp"),
            P(("grp", "dp", "kv"), None, "tp"),
            P(("grp", "dp", "kv"), None, "tp"),
            P(("grp", "dp", "kv")),
            P(("grp", "dp", "kv"), "tp", None, None),
            P("tp"),
            P("tp", "kv"),
            P(("kv", "tp")),
            P(("kv", "tp"), "dp"),
            P("dp", ("kv", "tp")),
        ),
        out_specs=P(("grp", "dp"), ("kv", "tp")),
        check_vma=False,
    )
```

```python
import jax
import jax.numpy as jnp
from jax import lax
from jax.sharding import Mesh
from jax.sharding import PartitionSpec as P

D = 4096
HEAD_DIM = 64
D_STATE = 128
TAPS = 4
SSM_WIDTH = 2048
LANES = 128
KV = ("kh", "kl")

EPS = 1e-06
BF16 = jnp.bfloat16
F32 = jnp.float32


def two_words(x):
    high = lax.reduce_precision(x, 8, 7)
    return high.astype(BF16), (x - high).astype(BF16)


def three_words(x):
    high = lax.reduce_precision(x, 8, 7)
    rest = x - high
    middle = lax.reduce_precision(rest, 8, 7)
    return high.astype(BF16), middle.astype(BF16), (rest - middle).astype(BF16)


def to_everyone(shard, axes):
    size = lax.axis_size(axes)
    return lax.all_to_all(
        jnp.broadcast_to(shard[None], (size, *shard.shape)), axes, 0, 0, tiled=True
    )


def from_partner(x, axis):
    size = lax.axis_size(axis)
    return lax.ppermute(x, axis, [(i, (i + 1) % size) for i in range(size)])


def exchanged(blocks, here, axes):
    team = blocks.shape[0]
    own = lax.dynamic_index_in_dim(blocks, here, 0, keepdims=True)
    out = jnp.zeros_like(blocks)
    out = lax.dynamic_update_slice_in_dim(out, own, here, 0)
    for mask in range(1, team):
        perm = [(i, i ^ mask) for i in range(team)]
        sent = lax.dynamic_index_in_dim(blocks, here ^ mask, 0, keepdims=True)
        got = lax.ppermute(sent, axes, perm)
        out = lax.dynamic_update_slice_in_dim(out, got, here ^ mask, 0)
    return out


def convolve(history, weights, newest):
    summed = weights[TAPS - 1] * newest
    for offset in range(TAPS - 1):
        summed = summed + weights[offset] * history[:, offset].astype(F32)
    return jax.nn.silu(summed)


def per_device(
    inputs,
    gain_in,
    w_gate,
    w_input,
    w_bproj,
    w_cproj,
    w_step,
    conv_input,
    conv_bproj,
    conv_cproj,
    tail_input,
    tail_bproj,
    tail_cproj,
    step_bias,
    decay_log,
    block_input,
    block_bproj,
    block_step,
    lengths,
    state,
    gain_mix,
    w_out,
    gain_mlp,
    w_up,
    w_down,
):
    core = lax.axis_index("tp")
    team = ("kl", "tp")
    member = lax.axis_index(team)
    n_team = lax.axis_size(team)
    n_kv, n_dp, n_tp = lax.axis_size(KV), lax.axis_size("dp"), lax.axis_size("tp")
    n_far = lax.axis_size("kh")
    stream = inputs.astype(F32)
    rows = inputs.shape[0]
    squares = jnp.sum(stream * stream, axis=1)
    scaled = (stream * gain_in).astype(BF16)
    matrices = (w_gate, w_input, w_bproj, w_cproj)
    pieces = [jnp.dot(scaled, weight, preferred_element_type=F32).astype(BF16) for weight in matrices]
    pieces += two_words(jnp.dot(scaled, w_step, preferred_element_type=F32))
    pieces += two_words(squares[:, None])
    bounds = [0]
    for piece in pieces:
        bounds.append(bounds[-1] + piece.shape[1])
    spare = -bounds[-1] % LANES
    pieces.append(jnp.zeros((rows, spare), BF16))
    sent = jnp.concatenate(pieces, axis=1).reshape(n_kv, rows // n_kv, -1)
    arrived = lax.all_to_all(sent, KV, 0, 0, tiled=True)

    out_blocks = jnp.moveaxis(w_out.reshape(w_out.shape[0], n_tp, -1), 1, 0)
    out_weight = exchanged(out_blocks, core, ("tp",)).reshape(-1, out_blocks.shape[2])
    up_blocks = jnp.moveaxis(w_up.reshape(w_up.shape[0], n_team, -1), 1, 0)
    depth, width = up_blocks.shape[1:]
    gain_words = jnp.stack(three_words(gain_mlp))
    gain_words = jnp.pad(gain_words, ((0, 5), (0, width - gain_words.shape[1])))
    up_blocks = jnp.concatenate(
        [up_blocks, jnp.broadcast_to(gain_words[None], (n_team, *gain_words.shape))], axis=1
    )
    up_blocks = exchanged(up_blocks, member, team)
    arrived, up_blocks = lax.optimization_barrier((arrived, up_blocks))
    projected = jnp.sum(arrived.astype(F32), axis=0)
    up_gain = jnp.sum(up_blocks[:, depth : depth + 3, : gain_mlp.shape[0]].astype(F32), axis=1)
    up_gain = up_gain.reshape(-1)
    up_weight = up_blocks[:, :depth].reshape(-1, width)
    down_blocks = w_down.reshape(n_team, -1, w_down.shape[1])
    down_weight = exchanged(down_blocks, member, team)

    parts = [projected[:, a:b] for a, b in zip(bounds[:-1], bounds[1:])]
    inverse = lax.rsqrt((parts[6] + parts[7]) / D + EPS)
    gate_pre, value_pre, b_pre, c_pre = [parts[k] * inverse for k in range(4)]
    step_pre = (parts[4] + parts[5]) * inverse
    seq_count = lengths.shape[0]
    head_count = step_bias.shape[0]
    group_count = w_bproj.shape[1] // D_STATE
    block_len = block_step.shape[1]
    per_group = head_count // group_count
    current = convolve(tail_input, conv_input, value_pre)
    b_now = convolve(tail_bproj, conv_bproj, b_pre)
    c_now = convolve(tail_cproj, conv_cproj, c_pre)
    step_size = jax.nn.softplus(step_pre + step_bias)
    decay_rate = -jnp.exp(decay_log)
    positions = lax.broadcasted_iota(jnp.int32, (1, block_len), 1)
    live_rows = (positions < lengths[:, None]).astype(F32)
    masked = block_step * live_rows[:, :, None]
    later_steps = jnp.sum(masked, axis=1, keepdims=True) - jnp.cumsum(masked, axis=1)
    decays = jnp.exp(decay_rate * (step_size[:, None, :] + later_steps)) * live_rows[:, :, None]
    c_query = c_now.astype(BF16).reshape(seq_count, group_count, D_STATE)
    keys = block_bproj.reshape(seq_count, block_len, group_count, D_STATE)
    scores = jnp.einsum("bsgn,bgn->bsg", keys, c_query, preferred_element_type=F32)
    scores = jnp.repeat(scores, per_group, axis=2)
    weights = (decays * scores * block_step).astype(BF16)
    values = block_input.reshape(seq_count, block_len, head_count, HEAD_DIM)
    inner_sum = jnp.einsum("bsh,bshp->bhp", weights, values, preferred_element_type=F32)
    c_full = c_now.reshape(seq_count, group_count, D_STATE)
    b_full = b_now.reshape(seq_count, group_count, D_STATE)
    own_score = jnp.repeat(jnp.sum(c_full * b_full, axis=2), per_group, axis=1)
    own_term = (step_size * own_score)[:, :, None] * current.reshape(
        seq_count, head_count, HEAD_DIM
    )
    carried = jnp.exp(decay_rate * (step_size + jnp.sum(masked, axis=1)))
    c_heads = jnp.repeat(c_full, per_group, axis=1)
    readout = jnp.einsum("bhpn,bhn->bhp", state, c_heads, precision=lax.Precision.HIGHEST)
    mixed = (inner_sum + own_term + carried[:, :, None] * readout).reshape(
        seq_count, -1
    ) * jax.nn.silu(gate_pre)

    width = mixed.shape[1]
    local_sq = two_words(jnp.sum(mixed * mixed, axis=1, keepdims=True))
    row = jnp.concatenate(
        [(mixed * gain_mix).astype(BF16), *local_sq, jnp.zeros((seq_count, LANES - 2), BF16)], axis=1
    )
    whole = to_everyone(row, KV + ("tp",)).reshape(n_kv, n_tp, seq_count, -1)
    whole = jnp.moveaxis(whole, 1, 0).reshape(n_tp, rows, -1)
    total_sq = jnp.sum(whole[:, :, width : width + 2].astype(F32), axis=(0, 2))
    channels = jnp.concatenate([whole[k, :, :width] for k in range(n_tp)], axis=1)
    mixed_in = jnp.dot(channels, out_weight, preferred_element_type=F32)
    mixed_in = mixed_in * lax.rsqrt(total_sq / SSM_WIDTH + EPS)[:, None]
    column_count = mixed_in.shape[1]
    residual = lax.dynamic_slice_in_dim(stream, core * column_count, column_count, 1)
    hidden = (residual + mixed_in).astype(BF16)

    all_hidden = to_everyone(hidden, ("dp",) + team).reshape(n_dp, n_team, rows, -1)
    all_hidden = jnp.moveaxis(all_hidden, 1, 2).reshape(n_dp * rows, -1).astype(F32)
    row_sq = jnp.sum(all_hidden * all_hidden, axis=1)
    lifted = (all_hidden * up_gain).astype(BF16)
    raised = lax.dot_general(
        up_weight, lifted, (((0,), (1,)), ((), ())), preferred_element_type=F32
    ).astype(BF16)
    seqs = raised.shape[1]
    extra = jnp.concatenate(
        [*[w[None] for w in two_words(row_sq)], jnp.zeros((6, seqs), BF16)], axis=0
    )
    sent = jnp.concatenate(
        [
            raised.reshape(n_far, -1, seqs),
            jnp.broadcast_to(extra[None], (n_far, *extra.shape)),
        ],
        axis=1,
    )
    arrived = lax.all_to_all(sent, "kh", 0, 0, tiled=True)
    arrived, down_weight = lax.optimization_barrier((arrived, down_weight))
    shares = jnp.sum(arrived.astype(F32), axis=0)
    unit_count = shares.shape[0] - 8
    sq_sum = shares[unit_count] + shares[unit_count + 1]
    units = jnp.square(
        jax.nn.relu(shares[:unit_count] * lax.rsqrt(sq_sum / D + EPS)[None, :])
    ).astype(BF16)
    hidden_units = to_everyone(units, "kh").reshape(-1, seqs)
    lowered = lax.dot_general(
        hidden_units, down_weight, (((0,), (1,)), ((), ())), preferred_element_type=F32
    ).astype(BF16)
    lowered = lowered.reshape(n_dp, rows, n_team, -1)
    lowered = jnp.moveaxis(lowered, 2, 1).reshape(n_dp * n_team, rows, -1)
    lowered = lax.all_to_all(lowered, ("dp",) + team, 0, 0, tiled=True)
    return (hidden.astype(F32) + jnp.sum(lowered.astype(F32), axis=0)).astype(BF16)


def solution(mesh):
    sizes = [mesh.shape[name] for name in ("grp", "dp", "kv", "tp")]
    pairs = mesh.devices.reshape(sizes[0], sizes[1], sizes[2] // 2, 2, sizes[3])
    mesh = Mesh(pairs, ("grp", "dp", "kh", "kl", "tp"))
    return jax.shard_map(
        per_device,
        mesh=mesh,
        in_specs=(
            P(("grp", "dp"), KV),
            P(KV),
            P(KV, "tp"),
            P(KV, "tp"),
            P(KV, "tp"),
            P(KV, "tp"),
            P(KV, "tp"),
            P(None, "tp"),
            P(None, "tp"),
            P(None, "tp"),
            P(("grp", "dp", *KV), None, "tp"),
            P(("grp", "dp", *KV), None, "tp"),
            P(("grp", "dp", *KV), None, "tp"),
            P("tp"),
            P("tp"),
            P(("grp", "dp", *KV), None, "tp"),
            P(("grp", "dp", *KV), None, "tp"),
            P(("grp", "dp", *KV), None, "tp"),
            P(("grp", "dp", *KV)),
            P(("grp", "dp", *KV), "tp", None, None),
            P("tp"),
            P("tp", KV),
            P((*KV, "tp")),
            P((*KV, "tp"), "dp"),
            P("dp", (*KV, "tp")),
        ),
        out_specs=P(("grp", "dp"), (*KV, "tp")),
        check_vma=False,
    )
```

```python
import jax
import jax.numpy as jnp
from jax import lax
from jax.experimental import pallas as pl
from jax.sharding import Mesh
from jax.sharding import PartitionSpec as P

D = 4096
HEAD_DIM = 64
D_STATE = 128
TAPS = 4
SSM_WIDTH = 2048
LANES = 128
KV = ("kh", "kl")

EPS = 1e-06
BF16 = jnp.bfloat16
F32 = jnp.float32


def two_words(x):
    high = lax.reduce_precision(x, 8, 7)
    return high.astype(BF16), (x - high).astype(BF16)


def three_words(x):
    high = lax.reduce_precision(x, 8, 7)
    rest = x - high
    middle = lax.reduce_precision(rest, 8, 7)
    return high.astype(BF16), middle.astype(BF16), (rest - middle).astype(BF16)


def to_everyone(shard, axes):
    size = lax.axis_size(axes)
    return lax.all_to_all(
        jnp.broadcast_to(shard[None], (size, *shard.shape)), axes, 0, 0, tiled=True
    )


def exchanged(blocks, here, axes):
    team = blocks.shape[0]
    own = lax.dynamic_index_in_dim(blocks, here, 0, keepdims=True)
    out = jnp.zeros_like(blocks)
    out = lax.dynamic_update_slice_in_dim(out, own, here, 0)
    for mask in range(1, team):
        perm = [(i, i ^ mask) for i in range(team)]
        sent = lax.dynamic_index_in_dim(blocks, here ^ mask, 0, keepdims=True)
        got = lax.ppermute(sent, axes, perm)
        out = lax.dynamic_update_slice_in_dim(out, got, here ^ mask, 0)
    return out


def project_body(x_ref, gain_ref, gate_ref, input_ref, b_ref, c_ref, step_ref, out_ref):
    stream = x_ref[...].astype(F32)
    scaled = (stream * gain_ref[...]).astype(BF16)
    dests, each = out_ref.shape[:2]
    at = 0

    def put(block):
        for k in range(dests):
            out_ref[k, :, at : at + block.shape[1]] = block[k * each : (k + 1) * each].astype(BF16)

    step = lax.dot_general(
        scaled, step_ref[...], (((1,), (1,)), ((), ())), preferred_element_type=F32
    )
    step_high = step.astype(BF16)
    step_low = (step - step_high.astype(F32)).astype(BF16)
    heads = step.shape[1]
    row = lax.broadcasted_iota(jnp.int32, (heads, LANES), 0)
    lane = lax.broadcasted_iota(jnp.int32, (heads, LANES), 1)
    tail = jnp.dot(step_high, (lane == row).astype(BF16), preferred_element_type=F32)
    tail += jnp.dot(step_low, (lane == row + heads).astype(BF16), preferred_element_type=F32)
    squares = jnp.sum(stream * stream, axis=1, keepdims=True)
    high = squares.astype(BF16).astype(F32)
    lane = lax.broadcasted_iota(jnp.int32, tail.shape, 1)
    tail += jnp.where(lane == 2 * heads, high, 0.0)
    tail += jnp.where(lane == 2 * heads + 1, squares - high, 0.0)
    for ref in (gate_ref, input_ref, b_ref, c_ref):
        put(jnp.dot(scaled, ref[...], preferred_element_type=F32))
        at += ref.shape[1]
    put(tail)


def project(inputs, gain_in, matrices, w_step, dests):
    rows = inputs.shape[0]
    width = sum(w.shape[1] for w in matrices) + LANES
    return pl.pallas_call(
        project_body,
        out_shape=jax.ShapeDtypeStruct((dests, rows // dests, width), BF16),
    )(inputs, gain_in[None], *matrices, w_step.T)


def convolve(history, weights, newest):
    summed = weights[TAPS - 1] * newest
    for offset in range(TAPS - 1):
        summed = summed + weights[offset] * history[:, offset].astype(F32)
    return jax.nn.silu(summed)


def layer(
    inputs,
    gain_in,
    w_gate,
    w_input,
    w_bproj,
    w_cproj,
    w_step,
    conv_input,
    conv_bproj,
    conv_cproj,
    tail_input,
    tail_bproj,
    tail_cproj,
    step_bias,
    decay_log,
    block_input,
    block_bproj,
    block_step,
    lengths,
    state,
    gain_mix,
    w_out,
    gain_mlp,
    w_up,
    w_down,
):
    core = lax.axis_index("tp")
    team = ("kl", "tp")
    member = lax.axis_index(team)
    n_team = lax.axis_size(team)
    n_kv, n_dp, n_tp = lax.axis_size(KV), lax.axis_size("dp"), lax.axis_size("tp")
    n_far = lax.axis_size("kh")
    stream = inputs.astype(F32)
    rows = inputs.shape[0]
    matrices = (w_gate, w_input, w_bproj, w_cproj)
    heads = w_step.shape[1]
    sent = project(inputs, gain_in, matrices, w_step, n_kv)
    bounds = [0]
    for width in [w.shape[1] for w in matrices] + [heads, heads, 1, 1]:
        bounds.append(bounds[-1] + width)
    arrived = lax.all_to_all(sent, KV, 0, 0, tiled=True)

    out_blocks = jnp.moveaxis(w_out.reshape(w_out.shape[0], n_tp, -1), 1, 0)
    out_weight = exchanged(out_blocks, core, ("tp",)).reshape(-1, out_blocks.shape[2])
    up_blocks = jnp.moveaxis(w_up.reshape(w_up.shape[0], n_team, -1), 1, 0)
    depth, width = up_blocks.shape[1:]
    gain_words = jnp.stack(three_words(gain_mlp))
    gain_words = jnp.pad(gain_words, ((0, 5), (0, width - gain_words.shape[1])))
    up_blocks = jnp.concatenate(
        [up_blocks, jnp.broadcast_to(gain_words[None], (n_team, *gain_words.shape))], axis=1
    )
    up_blocks = exchanged(up_blocks, member, team)
    arrived, up_blocks = lax.optimization_barrier((arrived, up_blocks))
    projected = jnp.sum(arrived.astype(F32), axis=0)
    up_gain = jnp.sum(up_blocks[:, depth : depth + 3, : gain_mlp.shape[0]].astype(F32), axis=1)
    up_gain = up_gain.reshape(-1)
    up_weight = up_blocks[:, :depth].reshape(-1, width)
    down_blocks = w_down.reshape(n_team, -1, w_down.shape[1])
    down_weight = exchanged(down_blocks, member, team)

    parts = [projected[:, a:b] for a, b in zip(bounds[:-1], bounds[1:])]
    inverse = lax.rsqrt((parts[6] + parts[7]) / D + EPS)
    gate_pre, value_pre, b_pre, c_pre = [parts[k] * inverse for k in range(4)]
    step_pre = (parts[4] + parts[5]) * inverse
    seq_count = lengths.shape[0]
    head_count = step_bias.shape[0]
    group_count = w_bproj.shape[1] // D_STATE
    block_len = block_step.shape[1]
    per_group = head_count // group_count
    current = convolve(tail_input, conv_input, value_pre)
    b_now = convolve(tail_bproj, conv_bproj, b_pre)
    c_now = convolve(tail_cproj, conv_cproj, c_pre)
    step_size = jax.nn.softplus(step_pre + step_bias)
    decay_rate = -jnp.exp(decay_log)
    positions = lax.broadcasted_iota(jnp.int32, (1, block_len), 1)
    live_rows = (positions < lengths[:, None]).astype(F32)
    masked = block_step * live_rows[:, :, None]
    later_steps = jnp.sum(masked, axis=1, keepdims=True) - jnp.cumsum(masked, axis=1)
    decays = jnp.exp(decay_rate * (step_size[:, None, :] + later_steps)) * live_rows[:, :, None]
    c_query = c_now.astype(BF16).reshape(seq_count, group_count, D_STATE)
    keys = block_bproj.reshape(seq_count, block_len, group_count, D_STATE)
    scores = jnp.einsum("bsgn,bgn->bsg", keys, c_query, preferred_element_type=F32)
    scores = jnp.repeat(scores, per_group, axis=2)
    weights = (decays * scores * block_step).astype(BF16)
    values = block_input.reshape(seq_count, block_len, head_count, HEAD_DIM)
    inner_sum = jnp.einsum("bsh,bshp->bhp", weights, values, preferred_element_type=F32)
    c_full = c_now.reshape(seq_count, group_count, D_STATE)
    b_full = b_now.reshape(seq_count, group_count, D_STATE)
    own_score = jnp.repeat(jnp.sum(c_full * b_full, axis=2), per_group, axis=1)
    own_term = (step_size * own_score)[:, :, None] * current.reshape(
        seq_count, head_count, HEAD_DIM
    )
    carried = jnp.exp(decay_rate * (step_size + jnp.sum(masked, axis=1)))
    c_heads = jnp.repeat(c_full, per_group, axis=1)
    readout = jnp.einsum("bhpn,bhn->bhp", state, c_heads, precision=lax.Precision.HIGHEST)
    mixed = (inner_sum + own_term + carried[:, :, None] * readout).reshape(
        seq_count, -1
    ) * jax.nn.silu(gate_pre)

    width = mixed.shape[1]
    local_sq = two_words(jnp.sum(mixed * mixed, axis=1, keepdims=True))
    row = jnp.concatenate(
        [(mixed * gain_mix).astype(BF16), *local_sq, jnp.zeros((seq_count, LANES - 2), BF16)], axis=1
    )
    whole = to_everyone(row, KV + ("tp",)).reshape(n_kv, n_tp, seq_count, -1)
    whole = jnp.moveaxis(whole, 1, 0).reshape(n_tp, rows, -1)
    total_sq = jnp.sum(whole[:, :, width : width + 2].astype(F32), axis=(0, 2))
    channels = jnp.concatenate([whole[k, :, :width] for k in range(n_tp)], axis=1)
    mixed_in = jnp.dot(channels, out_weight, preferred_element_type=F32)
    mixed_in = mixed_in * lax.rsqrt(total_sq / SSM_WIDTH + EPS)[:, None]
    column_count = mixed_in.shape[1]
    residual = lax.dynamic_slice_in_dim(stream, core * column_count, column_count, 1)
    hidden = (residual + mixed_in).astype(BF16)

    all_hidden = to_everyone(hidden, ("dp",) + team).reshape(n_dp, n_team, rows, -1)
    all_hidden = jnp.moveaxis(all_hidden, 1, 2).reshape(n_dp * rows, -1).astype(F32)
    row_sq = jnp.sum(all_hidden * all_hidden, axis=1)
    lifted = (all_hidden * up_gain).astype(BF16)
    raised = lax.dot_general(
        up_weight, lifted, (((0,), (1,)), ((), ())), preferred_element_type=F32
    ).astype(BF16)
    seqs = raised.shape[1]
    extra = jnp.concatenate(
        [*[w[None] for w in two_words(row_sq)], jnp.zeros((6, seqs), BF16)], axis=0
    )
    sent = jnp.concatenate(
        [
            raised.reshape(n_far, -1, seqs),
            jnp.broadcast_to(extra[None], (n_far, *extra.shape)),
        ],
        axis=1,
    )
    arrived = lax.all_to_all(sent, "kh", 0, 0, tiled=True)
    arrived, down_weight = lax.optimization_barrier((arrived, down_weight))
    shares = jnp.sum(arrived.astype(F32), axis=0)
    unit_count = shares.shape[0] - 8
    sq_sum = shares[unit_count] + shares[unit_count + 1]
    units = jnp.square(
        jax.nn.relu(shares[:unit_count] * lax.rsqrt(sq_sum / D + EPS)[None, :])
    ).astype(BF16)
    hidden_units = to_everyone(units, "kh").reshape(-1, seqs)
    lowered = lax.dot_general(
        hidden_units, down_weight, (((0,), (1,)), ((), ())), preferred_element_type=F32
    ).astype(BF16)
    lowered = lowered.reshape(n_dp, rows, n_team, -1)
    lowered = jnp.moveaxis(lowered, 2, 1).reshape(n_dp * n_team, rows, -1)
    lowered = lax.all_to_all(lowered, ("dp",) + team, 0, 0, tiled=True)
    return (hidden.astype(F32) + jnp.sum(lowered.astype(F32), axis=0)).astype(BF16)


def solution(mesh):
    sizes = [mesh.shape[name] for name in ("grp", "dp", "kv", "tp")]
    pairs = mesh.devices.reshape(sizes[0], sizes[1], sizes[2] // 2, 2, sizes[3])
    mesh = Mesh(pairs, ("grp", "dp", "kh", "kl", "tp"))
    return jax.shard_map(
        layer,
        mesh=mesh,
        in_specs=(
            P(("grp", "dp"), KV),
            P(KV),
            P(KV, "tp"),
            P(KV, "tp"),
            P(KV, "tp"),
            P(KV, "tp"),
            P(KV, "tp"),
            P(None, "tp"),
            P(None, "tp"),
            P(None, "tp"),
            P(("grp", "dp", *KV), None, "tp"),
            P(("grp", "dp", *KV), None, "tp"),
            P(("grp", "dp", *KV), None, "tp"),
            P("tp"),
            P("tp"),
            P(("grp", "dp", *KV), None, "tp"),
            P(("grp", "dp", *KV), None, "tp"),
            P(("grp", "dp", *KV), None, "tp"),
            P(("grp", "dp", *KV)),
            P(("grp", "dp", *KV), "tp", None, None),
            P("tp"),
            P("tp", KV),
            P((*KV, "tp")),
            P((*KV, "tp"), "dp"),
            P("dp", (*KV, "tp")),
        ),
        out_specs=P(("grp", "dp"), (*KV, "tp")),
        check_vma=False,
    )
```

```python
import jax
import jax.numpy as jnp
from jax import lax
from jax.experimental import pallas as pl
from jax.experimental.pallas import tpu as pltpu
from jax.sharding import PartitionSpec as P

D = 4096
HEAD_DIM = 64
TAPS = 4
SSM_WIDTH = 2048
LANES = 128
SPARE = 8

EPS = 1e-06
BF16 = jnp.bfloat16
F32 = jnp.float32


def two_words(x):
    high = lax.reduce_precision(x, 8, 7)
    return high.astype(BF16), (x - high).astype(BF16)


def to_everyone(shard, axes):
    size = lax.axis_size(axes)
    return lax.all_to_all(
        jnp.broadcast_to(shard[None], (size, *shard.shape)), axes, 0, 0, tiled=True
    )


def from_partner(x):
    size = lax.axis_size("tp")
    return lax.ppermute(x, "tp", [(i, (i + 1) % size) for i in range(size)])


def exchanged(weight, dim, core):
    half = weight.shape[dim] // 2
    mine = lax.dynamic_slice_in_dim(weight, core * half, half, dim)
    other = lax.dynamic_slice_in_dim(weight, (1 - core) * half, half, dim)
    return mine, from_partner(other)


def in_core_order(mine, other, core, dim):
    return jnp.where(
        core == 0,
        jnp.concatenate([mine, other], axis=dim),
        jnp.concatenate([other, mine], axis=dim),
    )


def contract_last(a, b):
    return lax.dot_general(a, b, (((1,), (1,)), ((), ())), preferred_element_type=F32)


def project_body(x_ref, gain_ref, gate_ref, input_ref, b_ref, c_ref, step_ref, out_ref):
    stream = x_ref[...].astype(F32)
    scaled = (stream * gain_ref[...]).astype(BF16)
    dests, each = out_ref.shape[:2]
    at = 0

    def put(block):
        for k in range(dests):
            out_ref[k, :, at : at + block.shape[1]] = block[k * each : (k + 1) * each].astype(BF16)

    step = contract_last(scaled, step_ref[...])
    step_high = step.astype(BF16)
    step_low = (step - step_high.astype(F32)).astype(BF16)
    heads = step.shape[1]
    row = lax.broadcasted_iota(jnp.int32, (heads, LANES), 0)
    lane = lax.broadcasted_iota(jnp.int32, (heads, LANES), 1)
    tail = jnp.dot(step_high, (lane == row).astype(BF16), preferred_element_type=F32)
    tail += jnp.dot(step_low, (lane == row + heads).astype(BF16), preferred_element_type=F32)
    squares = jnp.sum(stream * stream, axis=1, keepdims=True)
    high = squares.astype(BF16).astype(F32)
    lane = lax.broadcasted_iota(jnp.int32, tail.shape, 1)
    tail += jnp.where(lane == 2 * heads, high, 0.0)
    tail += jnp.where(lane == 2 * heads + 1, squares - high, 0.0)
    for ref in (gate_ref, input_ref, b_ref, c_ref):
        put(jnp.dot(scaled, ref[...], preferred_element_type=F32))
        at += ref.shape[1]
    put(tail)


def project(inputs, gain_in, matrices, w_step, dests):
    rows = inputs.shape[0]
    width = sum(w.shape[1] for w in matrices) + LANES
    return pl.pallas_call(
        project_body,
        out_shape=jax.ShapeDtypeStruct((dests, rows // dests, width), BF16),
    )(inputs, gain_in[None], *matrices, w_step.T)


def prepare_body(steps_ref, lengths_ref, log_ref, state_ref, faded_ref, all_ref, high_ref, low_ref):
    seqs, heads, block = steps_ref.shape
    rate = -jnp.exp(log_ref[...])
    position = lax.broadcasted_iota(jnp.int32, (heads, block), 1)
    after = lax.broadcasted_iota(jnp.int32, (block, block), 0) > lax.broadcasted_iota(
        jnp.int32, (block, block), 1
    )
    for b in range(seqs):
        masked = jnp.where(position < lengths_ref[b], steps_ref[b], 0.0)
        later = jnp.dot(
            masked, after.astype(F32), precision=lax.Precision.HIGHEST, preferred_element_type=F32
        )
        faded_ref[b] = jnp.exp(rate * later) * masked
        total = jnp.sum(masked, axis=1, keepdims=True)
        all_ref[b] = jnp.broadcast_to(jnp.exp(rate * total), (heads, block))
        high = state_ref[b].astype(BF16)
        high_ref[b] = high
        low_ref[b] = (state_ref[b] - high.astype(F32)).astype(BF16)


def prepare(block_step, lengths, decay_log, state):
    steps = jnp.swapaxes(block_step, 1, 2)
    flat = state.reshape(state.shape[0], -1, state.shape[3])
    shape = jax.ShapeDtypeStruct
    whole = pl.BlockSpec(memory_space=pltpu.VMEM)
    return pl.pallas_call(
        prepare_body,
        in_specs=[whole, pl.BlockSpec(memory_space=pltpu.SMEM), whole, whole],
        out_shape=(
            shape(steps.shape, F32),
            shape(steps.shape, F32),
            shape(flat.shape, BF16),
            shape(flat.shape, BF16),
        ),
    )(steps, lengths, decay_log[:, None], flat)


def on_chip(x):
    return pltpu.with_memory_space_constraint(x, pltpu.VMEM)


def silu(v):
    return v / (1.0 + jnp.exp(-v))


def mix_body(
    arrived_ref,
    conv_input_ref,
    conv_b_ref,
    conv_c_ref,
    tail_input_ref,
    tail_b_ref,
    tail_c_ref,
    bias_ref,
    log_ref,
    faded_ref,
    all_ref,
    high_ref,
    low_ref,
    values_ref,
    keys_ref,
    gain_ref,
    out_ref,
):
    seqs, heads = faded_ref.shape[:2]
    channels = gain_ref.shape[1]
    states = conv_c_ref.shape[1]
    n_state = high_ref.shape[2]
    per_group = heads * n_state // states
    total = jnp.sum(arrived_ref[...].astype(F32), axis=0)
    tail = total[:, 2 * channels + 2 * states :]
    lane = lax.broadcasted_iota(jnp.int32, tail.shape, 1)
    is_square = (lane == 2 * heads) | (lane == 2 * heads + 1)
    squares = jnp.sum(jnp.where(is_square, tail, 0.0), axis=1, keepdims=True)
    inverse = lax.rsqrt(squares / D + EPS)
    steps = (tail + pltpu.roll(tail, tail.shape[1] - heads, 1)) * inverse
    gate = silu(total[:, :channels] * inverse)

    def convolved(at, weights, history):
        summed = weights[TAPS - 1 :] * (total[:, at : at + weights.shape[1]] * inverse)
        for k in range(TAPS - 1):
            summed = summed + weights[k : k + 1] * history[k].astype(F32)
        return silu(summed)

    current = convolved(channels, conv_input_ref, tail_input_ref)
    b_now = convolved(2 * channels, conv_b_ref, tail_b_ref)
    c_now = convolved(2 * channels + states, conv_c_ref, tail_c_ref)

    rate = -jnp.exp(log_ref[...])
    head = lax.broadcasted_iota(jnp.int32, (heads, LANES), 0)
    column = lax.broadcasted_iota(jnp.int32, (heads, LANES), 1)
    key_head = lax.broadcasted_iota(jnp.int32, (heads, states), 0)
    key_lane = lax.broadcasted_iota(jnp.int32, (heads, states), 1)
    own_keys = key_lane // n_state == key_head // per_group
    out_head = lax.broadcasted_iota(jnp.int32, (heads, channels), 0)
    out_lane = lax.broadcasted_iota(jnp.int32, (heads, channels), 1)
    own_lanes = out_lane // HEAD_DIM == out_head
    head_state = lax.broadcasted_iota(jnp.int32, (heads, n_state), 0)

    def by_head(row):
        out = jnp.zeros((heads, n_state), F32)
        for g in range(states // n_state):
            part = row[:, g * n_state : (g + 1) * n_state]
            out = jnp.where(head_state // per_group == g, part, out)
        return out

    rows = []
    for b in range(seqs):
        one = slice(b, b + 1)
        step = jnp.sum(jnp.where(column == head, steps[one], 0.0), axis=1, keepdims=True)
        step = step + bias_ref[...]
        step = jnp.maximum(step, 0.0) + jnp.log1p(jnp.exp(-jnp.abs(step)))
        fade = jnp.exp(rate * step)
        query = jnp.where(own_keys, c_now[one], 0.0).astype(BF16)
        scores = contract_last(query, keys_ref[b])
        weights = (faded_ref[b] * fade * scores).astype(BF16)
        mixed = jnp.dot(weights, values_ref[b], preferred_element_type=F32)
        c_heads = by_head(c_now[one])
        c_high = c_heads.astype(BF16)
        c_low = (c_heads - c_high.astype(F32)).astype(BF16)
        readout = contract_last(c_high, high_ref[b])
        readout = readout + contract_last(c_low, high_ref[b])
        readout = readout + contract_last(c_high, low_ref[b])
        own = step * jnp.sum(c_heads * by_head(b_now[one]), axis=1, keepdims=True)
        carried = fade * all_ref[b][:, :1]
        mixed = mixed + carried * readout + own * current[one]
        rows.append(jnp.sum(jnp.where(own_lanes, mixed, 0.0), axis=0, keepdims=True))
    mixed = jnp.concatenate(rows, axis=0) * gate
    squares = jnp.sum(mixed * mixed, axis=1, keepdims=True)
    high = squares.astype(BF16).astype(F32)
    words = jnp.where(lane == 0, high, jnp.where(lane == 1, squares - high, 0.0))
    row = jnp.concatenate([mixed * gain_ref[...], words], axis=1).astype(BF16)
    for k in range(out_ref.shape[0]):
        out_ref[k] = row


def mix(arrived, convs, tails, step_bias, decay_log, prepared, values, keys, gain, copies):
    tails = [jnp.swapaxes(t, 0, 1) for t in tails]
    columns = (step_bias[:, None], decay_log[:, None])
    operands = (arrived, *convs, *tails, *columns, *prepared, values, keys, gain[None])
    width = gain.shape[0] + LANES
    return pl.pallas_call(
        mix_body,
        out_shape=jax.ShapeDtypeStruct((copies, values.shape[0], width), BF16),
    )(*[on_chip(x) for x in operands])


def layer(
    inputs,
    gain_in,
    w_gate,
    w_input,
    w_bproj,
    w_cproj,
    w_step,
    conv_input,
    conv_bproj,
    conv_cproj,
    tail_input,
    tail_bproj,
    tail_cproj,
    step_bias,
    decay_log,
    block_input,
    block_bproj,
    block_step,
    lengths,
    state,
    gain_mix,
    w_out,
    gain_mlp,
    w_up,
    w_down,
):
    core = lax.axis_index("tp")
    n_kv, n_dp, n_tp = lax.axis_size("kv"), lax.axis_size("dp"), lax.axis_size("tp")
    rows = inputs.shape[0]
    sent = project(inputs, gain_in, (w_gate, w_input, w_bproj, w_cproj), w_step, n_kv)
    arrived = lax.all_to_all(sent, "kv", 0, 0, tiled=True)
    prepared = prepare(block_step, lengths, decay_log, state)
    whole = mix(
        arrived,
        (conv_input, conv_bproj, conv_cproj),
        (tail_input, tail_bproj, tail_cproj),
        step_bias,
        decay_log,
        prepared,
        block_input,
        block_bproj,
        gain_mix,
        n_kv * n_tp,
    )
    width = gain_mix.shape[0]
    whole = lax.all_to_all(whole, ("kv", "tp"), 0, 0, tiled=True)

    out_mine, out_other = exchanged(w_out, 1, core)
    up_mine, up_other = exchanged(w_up, 1, core)
    up_gain = jnp.concatenate([gain_mlp, from_partner(gain_mlp)])
    column_count = out_mine.shape[1]
    residual = lax.dynamic_slice_in_dim(inputs, core * column_count, column_count, 1)
    whole, out_mine, out_other, up_mine, up_other, up_gain, residual = lax.optimization_barrier(
        (whole, out_mine, out_other, up_mine, up_other, up_gain, residual)
    )
    out_weight = jnp.concatenate([out_mine, out_other], axis=0)
    up_weight = jnp.concatenate([up_mine, up_other], axis=0)

    whole = whole.reshape(n_kv, n_tp, rows // n_kv, -1)
    whole = jnp.moveaxis(whole, 1, 0).reshape(n_tp, rows, -1)
    total_sq = jnp.sum(whole[:, :, width : width + 2].astype(F32), axis=(0, 2))
    halves = whole[:, :, :width]
    channels = jnp.concatenate(
        [
            lax.dynamic_index_in_dim(halves, core, 0, keepdims=False),
            lax.dynamic_index_in_dim(halves, 1 - core, 0, keepdims=False),
        ],
        axis=1,
    )
    mixed_in = jnp.dot(channels, out_weight, preferred_element_type=F32)
    mixed_in = mixed_in * lax.rsqrt(total_sq / SSM_WIDTH + EPS)[:, None]
    hidden = (residual.astype(F32) + mixed_in).astype(BF16)

    all_hidden = to_everyone(hidden, ("dp", "tp")).reshape(n_dp, n_tp, rows, -1)
    seqs = n_dp * rows
    all_hidden = jnp.moveaxis(all_hidden, 1, 0).reshape(n_tp, seqs, -1)
    all_hidden = jnp.concatenate(
        [
            lax.dynamic_index_in_dim(all_hidden, core, 0, keepdims=False),
            lax.dynamic_index_in_dim(all_hidden, 1 - core, 0, keepdims=False),
        ],
        axis=1,
    ).astype(F32)
    row_sq = jnp.sum(all_hidden * all_hidden, axis=1)
    lifted = (all_hidden * up_gain).astype(BF16)
    raised = lax.dot_general(
        up_weight, lifted, (((0,), (1,)), ((), ())), preferred_element_type=F32
    ).astype(BF16)
    arrived = lax.all_to_all(raised.reshape(n_kv, -1, seqs), "kv", 0, 0, tiled=True)
    down_mine, down_other = exchanged(w_down, 0, core)
    down_weight = in_core_order(down_mine, down_other, core, 1)
    down_weight = jnp.pad(down_weight.reshape(n_kv, -1, down_weight.shape[1]), ((0, 0), (0, SPARE), (0, 0)))
    down_weight = down_weight.reshape(-1, down_weight.shape[2])
    words = jnp.concatenate(
        [*[w[None] for w in two_words(row_sq)], jnp.zeros((SPARE - 2, seqs), BF16)], axis=0
    )
    arrived, down_weight, words = lax.optimization_barrier((arrived, down_weight, words))
    shares = jnp.sum(arrived.astype(F32), axis=0)
    units = jnp.square(jax.nn.relu(shares)).astype(BF16)
    hidden_units = lax.all_gather(jnp.concatenate([units, words], axis=0), "kv", axis=0, tiled=True)
    lowered = lax.dot_general(
        hidden_units, down_weight, (((0,), (0,)), ((), ())), preferred_element_type=F32
    ).astype(BF16)
    lowered = lowered.reshape(n_dp, rows, n_tp, -1)
    lowered = jnp.moveaxis(lowered, 2, 1).reshape(n_dp * n_tp, rows, -1)
    lowered = lax.all_to_all(lowered, ("dp", "tp"), 0, 0, tiled=True)
    lowered = jnp.sum(lowered.astype(F32), axis=0)
    unit_count = units.shape[0]
    sq_words = hidden_units.reshape(n_kv, -1, seqs)[:, unit_count : unit_count + 2]
    sq_sum = jnp.sum(sq_words.astype(F32), axis=(0, 1))
    sq_sum = lax.dynamic_slice_in_dim(sq_sum, lax.axis_index("dp") * rows, rows, 0)
    return (hidden.astype(F32) + lowered / (sq_sum / D + EPS)[:, None]).astype(BF16)


def solution(mesh):
    return jax.shard_map(
        layer,
        mesh=mesh,
        in_specs=(
            P(("grp", "dp"), "kv"),
            P("kv"),
            P("kv", "tp"),
            P("kv", "tp"),
            P("kv", "tp"),
            P("kv", "tp"),
            P("kv", "tp"),
            P(None, "tp"),
            P(None, "tp"),
            P(None, "tp"),
            P(("grp", "dp", "kv"), None, "tp"),
            P(("grp", "dp", "kv"), None, "tp"),
            P(("grp", "dp", "kv"), None, "tp"),
            P("tp"),
            P("tp"),
            P(("grp", "dp", "kv"), None, "tp"),
            P(("grp", "dp", "kv"), None, "tp"),
            P(("grp", "dp", "kv"), None, "tp"),
            P(("grp", "dp", "kv")),
            P(("grp", "dp", "kv"), "tp", None, None),
            P("tp"),
            P("tp", "kv"),
            P(("kv", "tp")),
            P(("kv", "tp"), "dp"),
            P("dp", ("kv", "tp")),
        ),
        out_specs=P(("grp", "dp"), ("kv", "tp")),
        check_vma=False,
    )
```

```python
import jax
import jax.numpy as jnp
from jax import lax
from jax.experimental import pallas as pl
from jax.experimental.pallas import tpu as pltpu
from jax.sharding import PartitionSpec as P

D = 4096
HEAD_DIM = 64
TAPS = 4
SSM_WIDTH = 2048
LANES = 128
SPARE = 8

EPS = 1e-06
BF16 = jnp.bfloat16
F32 = jnp.float32


def two_words(x):
    high = lax.reduce_precision(x, 8, 7)
    return high.astype(BF16), (x - high).astype(BF16)


def to_everyone(shard, axes):
    size = lax.axis_size(axes)
    return lax.all_to_all(
        jnp.broadcast_to(shard[None], (size, *shard.shape)), axes, 0, 0, tiled=True
    )


def from_partner(x):
    size = lax.axis_size("tp")
    return lax.ppermute(x, "tp", [(i, (i + 1) % size) for i in range(size)])


def exchanged(weight, dim, core):
    half = weight.shape[dim] // 2
    mine = lax.dynamic_slice_in_dim(weight, core * half, half, dim)
    other = lax.dynamic_slice_in_dim(weight, (1 - core) * half, half, dim)
    return mine, from_partner(other)


def in_core_order(mine, other, core, dim):
    return jnp.where(
        core == 0,
        jnp.concatenate([mine, other], axis=dim),
        jnp.concatenate([other, mine], axis=dim),
    )


def contract_last(a, b):
    return lax.dot_general(a, b, (((1,), (1,)), ((), ())), preferred_element_type=F32)


def project_body(x_ref, gain_ref, gate_ref, input_ref, b_ref, c_ref, step_ref, out_ref):
    stream = x_ref[...].astype(F32)
    scaled = (stream * gain_ref[...]).astype(BF16)
    dests, each = out_ref.shape[:2]
    at = 0

    def put(block):
        for k in range(dests):
            out_ref[k, :, at : at + block.shape[1]] = block[k * each : (k + 1) * each].astype(BF16)

    step = contract_last(scaled, step_ref[...])
    step_high = step.astype(BF16)
    step_low = (step - step_high.astype(F32)).astype(BF16)
    heads = step.shape[1]
    row = lax.broadcasted_iota(jnp.int32, (heads, LANES), 0)
    lane = lax.broadcasted_iota(jnp.int32, (heads, LANES), 1)
    tail = jnp.dot(step_high, (lane == row).astype(BF16), preferred_element_type=F32)
    tail += jnp.dot(step_low, (lane == row + heads).astype(BF16), preferred_element_type=F32)
    squares = jnp.sum(stream * stream, axis=1, keepdims=True)
    high = squares.astype(BF16).astype(F32)
    lane = lax.broadcasted_iota(jnp.int32, tail.shape, 1)
    tail += jnp.where(lane == 2 * heads, high, 0.0)
    tail += jnp.where(lane == 2 * heads + 1, squares - high, 0.0)
    for ref in (gate_ref, input_ref, b_ref, c_ref):
        put(jnp.dot(scaled, ref[...], preferred_element_type=F32))
        at += ref.shape[1]
    put(tail)


def project(inputs, gain_in, matrices, w_step, dests):
    rows = inputs.shape[0]
    width = sum(w.shape[1] for w in matrices) + LANES
    return pl.pallas_call(
        project_body,
        out_shape=jax.ShapeDtypeStruct((dests, rows // dests, width), BF16),
    )(inputs, gain_in[None], *matrices, w_step.T)


def prepare_body(steps_ref, lengths_ref, log_ref, state_ref, *refs):
    faded_ref, all_ref, high_ref, low_ref = refs[-4:]
    seqs, heads, block = steps_ref.shape
    rate = -jnp.exp(log_ref[...])
    position = lax.broadcasted_iota(jnp.int32, (heads, block), 1)
    after = lax.broadcasted_iota(jnp.int32, (block, block), 0) > lax.broadcasted_iota(
        jnp.int32, (block, block), 1
    )
    for b in range(seqs):
        masked = jnp.where(position < lengths_ref[b], steps_ref[b], 0.0)
        later = jnp.dot(
            masked, after.astype(F32), precision=lax.Precision.HIGHEST, preferred_element_type=F32
        )
        faded_ref[b] = jnp.exp(rate * later) * masked
        total = jnp.sum(masked, axis=1, keepdims=True)
        all_ref[b] = jnp.broadcast_to(jnp.exp(rate * total), (heads, block))
        high = state_ref[b].astype(BF16)
        high_ref[b] = high
        low_ref[b] = (state_ref[b] - high.astype(F32)).astype(BF16)


def prepare(block_step, lengths, log_column, state, others):
    steps = jnp.swapaxes(block_step, 1, 2)
    flat = state.reshape(state.shape[0], -1, state.shape[3])
    shape = pltpu.VMEM
    whole = pl.BlockSpec(memory_space=pltpu.VMEM)
    return pl.pallas_call(
        prepare_body,
        in_specs=[whole, pl.BlockSpec(memory_space=pltpu.SMEM)] + [whole] * (2 + len(others)),
        out_shape=(
            shape(steps.shape, F32),
            shape(steps.shape, F32),
            shape(flat.shape, BF16),
            shape(flat.shape, BF16),
        ),
    )(steps, lengths, log_column, flat, *others)


def on_chip(x):
    return pltpu.with_memory_space_constraint(x, pltpu.VMEM)


def silu(v):
    return v / (1.0 + jnp.exp(-v))


def mix_body(
    arrived_ref,
    conv_input_ref,
    conv_b_ref,
    conv_c_ref,
    tail_input_ref,
    tail_b_ref,
    tail_c_ref,
    bias_ref,
    log_ref,
    faded_ref,
    all_ref,
    high_ref,
    low_ref,
    values_ref,
    keys_ref,
    gain_ref,
    out_ref,
):
    seqs, heads = faded_ref.shape[:2]
    channels = gain_ref.shape[1]
    states = conv_c_ref.shape[1]
    n_state = high_ref.shape[2]
    per_group = heads * n_state // states
    total = jnp.sum(arrived_ref[...].astype(F32), axis=0)
    tail = total[:, 2 * channels + 2 * states :]
    lane = lax.broadcasted_iota(jnp.int32, tail.shape, 1)
    is_square = (lane == 2 * heads) | (lane == 2 * heads + 1)
    squares = jnp.sum(jnp.where(is_square, tail, 0.0), axis=1, keepdims=True)
    inverse = lax.rsqrt(squares / D + EPS)
    steps = (tail + pltpu.roll(tail, tail.shape[1] - heads, 1)) * inverse
    gate = silu(total[:, :channels] * inverse)

    def convolved(at, weights, history):
        summed = weights[TAPS - 1 :] * (total[:, at : at + weights.shape[1]] * inverse)
        for k in range(TAPS - 1):
            summed = summed + weights[k : k + 1] * history[k].astype(F32)
        return silu(summed)

    current = convolved(channels, conv_input_ref, tail_input_ref)
    b_now = convolved(2 * channels, conv_b_ref, tail_b_ref)
    c_now = convolved(2 * channels + states, conv_c_ref, tail_c_ref)

    rate = -jnp.exp(log_ref[...])
    head = lax.broadcasted_iota(jnp.int32, (heads, LANES), 0)
    column = lax.broadcasted_iota(jnp.int32, (heads, LANES), 1)
    key_head = lax.broadcasted_iota(jnp.int32, (heads, states), 0)
    key_lane = lax.broadcasted_iota(jnp.int32, (heads, states), 1)
    own_keys = key_lane // n_state == key_head // per_group
    out_head = lax.broadcasted_iota(jnp.int32, (heads, channels), 0)
    out_lane = lax.broadcasted_iota(jnp.int32, (heads, channels), 1)
    own_lanes = out_lane // HEAD_DIM == out_head
    head_state = lax.broadcasted_iota(jnp.int32, (heads, n_state), 0)

    def by_head(row):
        out = jnp.zeros((heads, n_state), F32)
        for g in range(states // n_state):
            part = row[:, g * n_state : (g + 1) * n_state]
            out = jnp.where(head_state // per_group == g, part, out)
        return out

    rows = []
    for b in range(seqs):
        one = slice(b, b + 1)
        step = jnp.sum(jnp.where(column == head, steps[one], 0.0), axis=1, keepdims=True)
        step = step + bias_ref[...]
        step = jnp.maximum(step, 0.0) + jnp.log1p(jnp.exp(-jnp.abs(step)))
        fade = jnp.exp(rate * step)
        query = jnp.where(own_keys, c_now[one], 0.0).astype(BF16)
        scores = contract_last(query, keys_ref[b])
        weights = (faded_ref[b] * fade * scores).astype(BF16)
        mixed = jnp.dot(weights, values_ref[b], preferred_element_type=F32)
        c_heads = by_head(c_now[one])
        c_high = c_heads.astype(BF16)
        c_low = (c_heads - c_high.astype(F32)).astype(BF16)
        readout = contract_last(c_high, high_ref[b])
        readout = readout + contract_last(c_low, high_ref[b])
        readout = readout + contract_last(c_high, low_ref[b])
        own = step * jnp.sum(c_heads * by_head(b_now[one]), axis=1, keepdims=True)
        carried = fade * all_ref[b][:, :1]
        mixed = mixed + carried * readout + own * current[one]
        rows.append(jnp.sum(jnp.where(own_lanes, mixed, 0.0), axis=0, keepdims=True))
    mixed = jnp.concatenate(rows, axis=0) * gate
    squares = jnp.sum(mixed * mixed, axis=1, keepdims=True)
    high = squares.astype(BF16).astype(F32)
    words = jnp.where(lane == 0, high, jnp.where(lane == 1, squares - high, 0.0))
    row = jnp.concatenate([mixed * gain_ref[...], words], axis=1).astype(BF16)
    for k in range(out_ref.shape[0]):
        out_ref[k] = row


def mix(arrived, convs, tails, columns, prepared, values, keys, gain, copies):
    operands = (on_chip(arrived), *convs, *tails, *columns, *[on_chip(x) for x in prepared])
    operands += (values, keys, gain)
    width = gain.shape[1] + LANES
    return pl.pallas_call(
        mix_body,
        out_shape=jax.ShapeDtypeStruct((copies, values.shape[0], width), BF16),
    )(*operands)


def layer(
    inputs,
    gain_in,
    w_gate,
    w_input,
    w_bproj,
    w_cproj,
    w_step,
    conv_input,
    conv_bproj,
    conv_cproj,
    tail_input,
    tail_bproj,
    tail_cproj,
    step_bias,
    decay_log,
    block_input,
    block_bproj,
    block_step,
    lengths,
    state,
    gain_mix,
    w_out,
    gain_mlp,
    w_up,
    w_down,
):
    core = lax.axis_index("tp")
    n_kv, n_dp, n_tp = lax.axis_size("kv"), lax.axis_size("dp"), lax.axis_size("tp")
    rows = inputs.shape[0]
    sent = project(inputs, gain_in, (w_gate, w_input, w_bproj, w_cproj), w_step, n_kv)
    arrived = lax.all_to_all(sent, "kv", 0, 0, tiled=True)
    convs = [on_chip(x) for x in (conv_input, conv_bproj, conv_cproj)]
    tails = [on_chip(jnp.swapaxes(x, 0, 1)) for x in (tail_input, tail_bproj, tail_cproj)]
    columns = [on_chip(x[:, None]) for x in (step_bias, decay_log)]
    values, keys, gain = [on_chip(x) for x in (block_input, block_bproj, gain_mix[None])]
    others = (*convs, *tails, columns[0], values, keys, gain)
    prepared = prepare(block_step, lengths, columns[1], state, others)
    whole = mix(arrived, convs, tails, columns, prepared, values, keys, gain, n_kv * n_tp)
    width = gain_mix.shape[0]
    whole = lax.all_to_all(whole, ("kv", "tp"), 0, 0, tiled=True)

    out_mine, out_other = exchanged(w_out, 1, core)
    up_mine, up_other = exchanged(w_up, 1, core)
    up_gain = jnp.concatenate([gain_mlp, from_partner(gain_mlp)])
    column_count = out_mine.shape[1]
    residual = lax.dynamic_slice_in_dim(inputs, core * column_count, column_count, 1)
    whole, out_mine, out_other, up_mine, up_other, up_gain, residual = lax.optimization_barrier(
        (whole, out_mine, out_other, up_mine, up_other, up_gain, residual)
    )
    out_weight = jnp.concatenate([out_mine, out_other], axis=0)
    up_weight = jnp.concatenate([up_mine, up_other], axis=0)

    whole = whole.reshape(n_kv, n_tp, rows // n_kv, -1)
    whole = jnp.moveaxis(whole, 1, 0).reshape(n_tp, rows, -1)
    total_sq = jnp.sum(whole[:, :, width : width + 2].astype(F32), axis=(0, 2))
    halves = whole[:, :, :width]
    channels = jnp.concatenate(
        [
            lax.dynamic_index_in_dim(halves, core, 0, keepdims=False),
            lax.dynamic_index_in_dim(halves, 1 - core, 0, keepdims=False),
        ],
        axis=1,
    )
    mixed_in = jnp.dot(channels, out_weight, preferred_element_type=F32)
    mixed_in = mixed_in * lax.rsqrt(total_sq / SSM_WIDTH + EPS)[:, None]
    hidden = (residual.astype(F32) + mixed_in).astype(BF16)

    all_hidden = to_everyone(hidden, ("dp", "tp")).reshape(n_dp, n_tp, rows, -1)
    seqs = n_dp * rows
    all_hidden = jnp.moveaxis(all_hidden, 1, 0).reshape(n_tp, seqs, -1)
    all_hidden = jnp.concatenate(
        [
            lax.dynamic_index_in_dim(all_hidden, core, 0, keepdims=False),
            lax.dynamic_index_in_dim(all_hidden, 1 - core, 0, keepdims=False),
        ],
        axis=1,
    ).astype(F32)
    row_sq = jnp.sum(all_hidden * all_hidden, axis=1)
    lifted = (all_hidden * up_gain).astype(BF16)
    raised = lax.dot_general(
        up_weight, lifted, (((0,), (1,)), ((), ())), preferred_element_type=F32
    ).astype(BF16)
    arrived = lax.all_to_all(raised.reshape(n_kv, -1, seqs), "kv", 0, 0, tiled=True)
    down_mine, down_other = exchanged(w_down, 0, core)
    down_weight = in_core_order(down_mine, down_other, core, 1)
    down_weight = jnp.pad(down_weight.reshape(n_kv, -1, down_weight.shape[1]), ((0, 0), (0, SPARE), (0, 0)))
    down_weight = down_weight.reshape(-1, down_weight.shape[2])
    words = jnp.concatenate(
        [*[w[None] for w in two_words(row_sq)], jnp.zeros((SPARE - 2, seqs), BF16)], axis=0
    )
    arrived, down_weight, words = lax.optimization_barrier((arrived, down_weight, words))
    shares = jnp.sum(arrived.astype(F32), axis=0)
    units = jnp.square(jax.nn.relu(shares)).astype(BF16)
    hidden_units = lax.all_gather(jnp.concatenate([units, words], axis=0), "kv", axis=0, tiled=True)
    lowered = lax.dot_general(
        hidden_units, down_weight, (((0,), (0,)), ((), ())), preferred_element_type=F32
    ).astype(BF16)
    lowered = lowered.reshape(n_dp, rows, n_tp, -1)
    lowered = jnp.moveaxis(lowered, 2, 1).reshape(n_dp * n_tp, rows, -1)
    lowered = lax.all_to_all(lowered, ("dp", "tp"), 0, 0, tiled=True)
    lowered = jnp.sum(lowered.astype(F32), axis=0)
    unit_count = units.shape[0]
    sq_words = hidden_units.reshape(n_kv, -1, seqs)[:, unit_count : unit_count + 2]
    sq_sum = jnp.sum(sq_words.astype(F32), axis=(0, 1))
    sq_sum = lax.dynamic_slice_in_dim(sq_sum, lax.axis_index("dp") * rows, rows, 0)
    return (hidden.astype(F32) + lowered / (sq_sum / D + EPS)[:, None]).astype(BF16)


def solution(mesh):
    return jax.shard_map(
        layer,
        mesh=mesh,
        in_specs=(
            P(("grp", "dp"), "kv"),
            P("kv"),
            P("kv", "tp"),
            P("kv", "tp"),
            P("kv", "tp"),
            P("kv", "tp"),
            P("kv", "tp"),
            P(None, "tp"),
            P(None, "tp"),
            P(None, "tp"),
            P(("grp", "dp", "kv"), None, "tp"),
            P(("grp", "dp", "kv"), None, "tp"),
            P(("grp", "dp", "kv"), None, "tp"),
            P("tp"),
            P("tp"),
            P(("grp", "dp", "kv"), None, "tp"),
            P(("grp", "dp", "kv"), None, "tp"),
            P(("grp", "dp", "kv"), None, "tp"),
            P(("grp", "dp", "kv")),
            P(("grp", "dp", "kv"), "tp", None, None),
            P("tp"),
            P("tp", "kv"),
            P(("kv", "tp")),
            P(("kv", "tp"), "dp"),
            P("dp", ("kv", "tp")),
        ),
        out_specs=P(("grp", "dp"), ("kv", "tp")),
        check_vma=False,
    )
```

```python
import jax
import jax.numpy as jnp
from jax import lax
from jax.experimental import pallas as pl
from jax.experimental.pallas import tpu as pltpu
from jax.sharding import Mesh
from jax.sharding import PartitionSpec as P

D = 4096
HEAD_DIM = 64
TAPS = 4
SSM_WIDTH = 2048
LANES = 128
SPARE = 8
KV = ("kh", "kl")
TEAM = ("kl", "tp")

EPS = 1e-06
BF16 = jnp.bfloat16
F32 = jnp.float32


def two_words(x):
    high = lax.reduce_precision(x, 8, 7)
    return high.astype(BF16), (x - high).astype(BF16)


def to_everyone(shard, axes):
    size = lax.axis_size(axes)
    return lax.all_to_all(
        jnp.broadcast_to(shard[None], (size, *shard.shape)), axes, 0, 0, tiled=True
    )


def swapped(array, dim, here, axis):
    half = array.shape[dim] // 2
    size = lax.axis_size(axis)
    mine = lax.dynamic_slice_in_dim(array, here * half, half, dim)
    other = lax.dynamic_slice_in_dim(array, (1 - here) * half, half, dim)
    return mine, lax.ppermute(other, axis, [(i, (i + 1) % size) for i in range(size)])


def in_order(mine, other, here, dim):
    return jnp.where(
        here == 0,
        jnp.concatenate([mine, other], axis=dim),
        jnp.concatenate([other, mine], axis=dim),
    )


def contract_last(a, b):
    return lax.dot_general(a, b, (((1,), (1,)), ((), ())), preferred_element_type=F32)


def project_body(x_ref, gain_ref, gate_ref, input_ref, b_ref, c_ref, step_ref, out_ref):
    stream = x_ref[...].astype(F32)
    scaled = (stream * gain_ref[...]).astype(BF16)
    dests, each = out_ref.shape[:2]
    at = 0

    def put(block):
        for k in range(dests):
            out_ref[k, :, at : at + block.shape[1]] = block[k * each : (k + 1) * each].astype(BF16)

    step = contract_last(scaled, step_ref[...])
    step_high = step.astype(BF16)
    step_low = (step - step_high.astype(F32)).astype(BF16)
    heads = step.shape[1]
    row = lax.broadcasted_iota(jnp.int32, (heads, LANES), 0)
    lane = lax.broadcasted_iota(jnp.int32, (heads, LANES), 1)
    tail = jnp.dot(step_high, (lane == row).astype(BF16), preferred_element_type=F32)
    tail += jnp.dot(step_low, (lane == row + heads).astype(BF16), preferred_element_type=F32)
    squares = jnp.sum(stream * stream, axis=1, keepdims=True)
    high = squares.astype(BF16).astype(F32)
    lane = lax.broadcasted_iota(jnp.int32, tail.shape, 1)
    tail += jnp.where(lane == 2 * heads, high, 0.0)
    tail += jnp.where(lane == 2 * heads + 1, squares - high, 0.0)
    for ref in (gate_ref, input_ref, b_ref, c_ref):
        put(jnp.dot(scaled, ref[...], preferred_element_type=F32))
        at += ref.shape[1]
    put(tail)


def project(inputs, gain_in, matrices, w_step, dests):
    rows = inputs.shape[0]
    width = sum(w.shape[1] for w in matrices) + LANES
    return pl.pallas_call(
        project_body,
        out_shape=jax.ShapeDtypeStruct((dests, rows // dests, width), BF16),
    )(inputs, gain_in[None], *matrices, w_step.T)


def prepare_body(steps_ref, lengths_ref, log_ref, state_ref, *refs):
    faded_ref, all_ref, high_ref, low_ref = refs[-4:]
    seqs, heads, block = steps_ref.shape
    rate = -jnp.exp(log_ref[...])
    position = lax.broadcasted_iota(jnp.int32, (heads, block), 1)
    after = lax.broadcasted_iota(jnp.int32, (block, block), 0) > lax.broadcasted_iota(
        jnp.int32, (block, block), 1
    )
    for b in range(seqs):
        masked = jnp.where(position < lengths_ref[b], steps_ref[b], 0.0)
        later = jnp.dot(
            masked, after.astype(F32), precision=lax.Precision.HIGHEST, preferred_element_type=F32
        )
        faded_ref[b] = jnp.exp(rate * later) * masked
        total = jnp.sum(masked, axis=1, keepdims=True)
        all_ref[b] = jnp.broadcast_to(jnp.exp(rate * total), (heads, block))
        high = state_ref[b].astype(BF16)
        high_ref[b] = high
        low_ref[b] = (state_ref[b] - high.astype(F32)).astype(BF16)


def prepare(block_step, lengths, log_column, state, others):
    steps = jnp.swapaxes(block_step, 1, 2)
    flat = state.reshape(state.shape[0], -1, state.shape[3])
    shape = pltpu.VMEM
    whole = pl.BlockSpec(memory_space=pltpu.VMEM)
    return pl.pallas_call(
        prepare_body,
        in_specs=[whole, pl.BlockSpec(memory_space=pltpu.SMEM)] + [whole] * (2 + len(others)),
        out_shape=(
            shape(steps.shape, F32),
            shape(steps.shape, F32),
            shape(flat.shape, BF16),
            shape(flat.shape, BF16),
        ),
    )(steps, lengths, log_column, flat, *others)


def on_chip(x):
    return pltpu.with_memory_space_constraint(x, pltpu.VMEM)


def silu(v):
    return v / (1.0 + jnp.exp(-v))


def mix_body(
    arrived_ref,
    conv_input_ref,
    conv_b_ref,
    conv_c_ref,
    tail_input_ref,
    tail_b_ref,
    tail_c_ref,
    bias_ref,
    log_ref,
    faded_ref,
    all_ref,
    high_ref,
    low_ref,
    values_ref,
    keys_ref,
    gain_ref,
    out_ref,
):
    seqs, heads = faded_ref.shape[:2]
    channels = gain_ref.shape[1]
    states = conv_c_ref.shape[1]
    n_state = high_ref.shape[2]
    per_group = heads * n_state // states
    total = jnp.sum(arrived_ref[...].astype(F32), axis=0)
    tail = total[:, 2 * channels + 2 * states :]
    lane = lax.broadcasted_iota(jnp.int32, tail.shape, 1)
    is_square = (lane == 2 * heads) | (lane == 2 * heads + 1)
    squares = jnp.sum(jnp.where(is_square, tail, 0.0), axis=1, keepdims=True)
    inverse = lax.rsqrt(squares / D + EPS)
    steps = (tail + pltpu.roll(tail, tail.shape[1] - heads, 1)) * inverse
    gate = silu(total[:, :channels] * inverse)

    def convolved(at, weights, history):
        summed = weights[TAPS - 1 :] * (total[:, at : at + weights.shape[1]] * inverse)
        for k in range(TAPS - 1):
            summed = summed + weights[k : k + 1] * history[k].astype(F32)
        return silu(summed)

    current = convolved(channels, conv_input_ref, tail_input_ref)
    b_now = convolved(2 * channels, conv_b_ref, tail_b_ref)
    c_now = convolved(2 * channels + states, conv_c_ref, tail_c_ref)

    rate = -jnp.exp(log_ref[...])
    head = lax.broadcasted_iota(jnp.int32, (heads, LANES), 0)
    column = lax.broadcasted_iota(jnp.int32, (heads, LANES), 1)
    key_head = lax.broadcasted_iota(jnp.int32, (heads, states), 0)
    key_lane = lax.broadcasted_iota(jnp.int32, (heads, states), 1)
    own_keys = key_lane // n_state == key_head // per_group
    out_head = lax.broadcasted_iota(jnp.int32, (heads, channels), 0)
    out_lane = lax.broadcasted_iota(jnp.int32, (heads, channels), 1)
    own_lanes = out_lane // HEAD_DIM == out_head
    head_state = lax.broadcasted_iota(jnp.int32, (heads, n_state), 0)

    def by_head(row):
        out = jnp.zeros((heads, n_state), F32)
        for g in range(states // n_state):
            part = row[:, g * n_state : (g + 1) * n_state]
            out = jnp.where(head_state // per_group == g, part, out)
        return out

    rows = []
    for b in range(seqs):
        one = slice(b, b + 1)
        step = jnp.sum(jnp.where(column == head, steps[one], 0.0), axis=1, keepdims=True)
        step = step + bias_ref[...]
        step = jnp.maximum(step, 0.0) + jnp.log1p(jnp.exp(-jnp.abs(step)))
        fade = jnp.exp(rate * step)
        query = jnp.where(own_keys, c_now[one], 0.0).astype(BF16)
        scores = contract_last(query, keys_ref[b])
        weights = (faded_ref[b] * fade * scores).astype(BF16)
        mixed = jnp.dot(weights, values_ref[b], preferred_element_type=F32)
        c_heads = by_head(c_now[one])
        c_high = c_heads.astype(BF16)
        c_low = (c_heads - c_high.astype(F32)).astype(BF16)
        readout = contract_last(c_high, high_ref[b])
        readout = readout + contract_last(c_low, high_ref[b])
        readout = readout + contract_last(c_high, low_ref[b])
        own = step * jnp.sum(c_heads * by_head(b_now[one]), axis=1, keepdims=True)
        carried = fade * all_ref[b][:, :1]
        mixed = mixed + carried * readout + own * current[one]
        rows.append(jnp.sum(jnp.where(own_lanes, mixed, 0.0), axis=0, keepdims=True))
    mixed = jnp.concatenate(rows, axis=0) * gate
    squares = jnp.sum(mixed * mixed, axis=1, keepdims=True)
    high = squares.astype(BF16).astype(F32)
    words = jnp.where(lane == 0, high, jnp.where(lane == 1, squares - high, 0.0))
    row = jnp.concatenate([mixed * gain_ref[...], words], axis=1).astype(BF16)
    for k in range(out_ref.shape[0]):
        out_ref[k] = row


def mix(arrived, convs, tails, columns, prepared, values, keys, gain, copies):
    operands = (on_chip(arrived), *convs, *tails, *columns, *[on_chip(x) for x in prepared])
    operands += (values, keys, gain)
    width = gain.shape[1] + LANES
    return pl.pallas_call(
        mix_body,
        out_shape=jax.ShapeDtypeStruct((copies, values.shape[0], width), BF16),
    )(*operands)


def layer(
    inputs,
    gain_in,
    w_gate,
    w_input,
    w_bproj,
    w_cproj,
    w_step,
    conv_input,
    conv_bproj,
    conv_cproj,
    tail_input,
    tail_bproj,
    tail_cproj,
    step_bias,
    decay_log,
    block_input,
    block_bproj,
    block_step,
    lengths,
    state,
    gain_mix,
    w_out,
    gain_mlp,
    w_up,
    w_down,
):
    core = lax.axis_index("tp")
    side = lax.axis_index("kl")
    n_kv, n_dp, n_tp = lax.axis_size(KV), lax.axis_size("dp"), lax.axis_size("tp")
    n_far, n_team = lax.axis_size("kh"), lax.axis_size(TEAM)
    rows = inputs.shape[0]
    sent = project(inputs, gain_in, (w_gate, w_input, w_bproj, w_cproj), w_step, n_kv)
    arrived = lax.all_to_all(sent, KV, 0, 0, tiled=True)
    convs = [on_chip(x) for x in (conv_input, conv_bproj, conv_cproj)]
    tails = [on_chip(jnp.swapaxes(x, 0, 1)) for x in (tail_input, tail_bproj, tail_cproj)]
    columns = [on_chip(x[:, None]) for x in (step_bias, decay_log)]
    values, keys, gain = [on_chip(x) for x in (block_input, block_bproj, gain_mix[None])]
    others = (*convs, *tails, columns[0], values, keys, gain)
    prepared = prepare(block_step, lengths, columns[1], state, others)
    scaled_up = (w_up.astype(F32) * gain_mlp[:, None]).astype(BF16)
    up_mine, up_other = swapped(scaled_up, 1, core, "tp")
    up_half = in_order(up_mine, up_other, core, 0)
    arrived, up_half = lax.optimization_barrier((arrived, up_half))
    whole = mix(arrived, convs, tails, columns, prepared, values, keys, gain, n_kv * n_tp)
    width = gain_mix.shape[0]
    whole = lax.all_to_all(whole, (*KV, "tp"), 0, 0, tiled=True)

    out_mine, out_other = swapped(w_out, 1, core, "tp")
    up_mine, up_other = swapped(up_half, 1, side, "kl")
    up_weight = in_order(up_mine, up_other, side, 0)
    column_count = out_mine.shape[1]
    residual = lax.dynamic_slice_in_dim(inputs, core * column_count, column_count, 1)
    whole, out_mine, out_other, up_weight, residual = lax.optimization_barrier(
        (whole, out_mine, out_other, up_weight, residual)
    )
    out_weight = jnp.concatenate([out_mine, out_other], axis=0)

    whole = whole.reshape(n_kv, n_tp, rows // n_kv, -1)
    whole = jnp.moveaxis(whole, 1, 0).reshape(n_tp, rows, -1)
    total_sq = jnp.sum(whole[:, :, width : width + 2].astype(F32), axis=(0, 2))
    halves = whole[:, :, :width]
    channels = jnp.concatenate(
        [
            lax.dynamic_index_in_dim(halves, core, 0, keepdims=False),
            lax.dynamic_index_in_dim(halves, 1 - core, 0, keepdims=False),
        ],
        axis=1,
    )
    mixed_in = jnp.dot(channels, out_weight, preferred_element_type=F32)
    mixed_in = mixed_in * lax.rsqrt(total_sq / SSM_WIDTH + EPS)[:, None]
    hidden = (residual.astype(F32) + mixed_in).astype(BF16)

    all_hidden = to_everyone(hidden, ("dp", *TEAM)).reshape(n_dp, n_team, rows, -1)
    seqs = n_dp * rows
    all_hidden = jnp.moveaxis(all_hidden, 1, 2).reshape(seqs, -1)
    raised = lax.dot_general(
        up_weight, all_hidden, (((0,), (1,)), ((), ())), preferred_element_type=F32
    ).astype(BF16)
    row_sq = jnp.sum(jnp.square(all_hidden.astype(F32)), axis=1)
    arrived = lax.all_to_all(raised.reshape(n_far, -1, seqs), "kh", 0, 0, tiled=True)
    down_half = in_order(*swapped(w_down, 0, core, "tp"), core, 1)
    down_weight = in_order(*swapped(down_half, 0, side, "kl"), side, 1)
    down_weight = down_weight.reshape(n_far, -1, down_weight.shape[1])
    down_weight = jnp.pad(down_weight, ((0, 0), (0, SPARE), (0, 0)))
    down_weight = down_weight.reshape(-1, down_weight.shape[2])
    words = jnp.concatenate(
        [*[w[None] for w in two_words(row_sq)], jnp.zeros((SPARE - 2, seqs), BF16)], axis=0
    )
    arrived, down_weight, words = lax.optimization_barrier((arrived, down_weight, words))
    shares = jnp.sum(arrived.astype(F32), axis=0)
    units = jnp.square(jax.nn.relu(shares)).astype(BF16)
    hidden_units = to_everyone(jnp.concatenate([units, words], axis=0), "kh")
    hidden_units = hidden_units.reshape(-1, seqs)
    lowered = lax.dot_general(
        hidden_units, down_weight, (((0,), (0,)), ((), ())), preferred_element_type=F32
    ).astype(BF16)
    lowered = lowered.reshape(n_dp, rows, n_team, -1)
    lowered = jnp.moveaxis(lowered, 2, 1).reshape(n_dp * n_team, rows, -1)
    lowered = lax.all_to_all(lowered, ("dp", *TEAM), 0, 0, tiled=True)
    lowered = jnp.sum(lowered.astype(F32), axis=0)
    unit_count = units.shape[0]
    sq_words = hidden_units.reshape(n_far, -1, seqs)[:, unit_count : unit_count + 2]
    sq_sum = jnp.sum(sq_words.astype(F32), axis=(0, 1))
    sq_sum = lax.dynamic_slice_in_dim(sq_sum, lax.axis_index("dp") * rows, rows, 0)
    return (hidden.astype(F32) + lowered / (sq_sum / D + EPS)[:, None]).astype(BF16)


def solution(mesh):
    sizes = [mesh.shape[name] for name in ("grp", "dp", "kv", "tp")]
    pairs = mesh.devices.reshape(sizes[0], sizes[1], sizes[2] // 2, 2, sizes[3])
    mesh = Mesh(pairs, ("grp", "dp", "kh", "kl", "tp"))
    return jax.shard_map(
        layer,
        mesh=mesh,
        in_specs=(
            P(("grp", "dp"), KV),
            P(KV),
            P(KV, "tp"),
            P(KV, "tp"),
            P(KV, "tp"),
            P(KV, "tp"),
            P(KV, "tp"),
            P(None, "tp"),
            P(None, "tp"),
            P(None, "tp"),
            P(("grp", "dp", *KV), None, "tp"),
            P(("grp", "dp", *KV), None, "tp"),
            P(("grp", "dp", *KV), None, "tp"),
            P("tp"),
            P("tp"),
            P(("grp", "dp", *KV), None, "tp"),
            P(("grp", "dp", *KV), None, "tp"),
            P(("grp", "dp", *KV), None, "tp"),
            P(("grp", "dp", *KV)),
            P(("grp", "dp", *KV), "tp", None, None),
            P("tp"),
            P("tp", KV),
            P((*KV, "tp")),
            P((*KV, "tp"), "dp"),
            P("dp", (*KV, "tp")),
        ),
        out_specs=P(("grp", "dp"), (*KV, "tp")),
        check_vma=False,
    )
```

```python
import jax
import jax.numpy as jnp
from jax import lax
from jax.experimental import pallas as pl
from jax.experimental.pallas import tpu as pltpu
from jax.sharding import Mesh
from jax.sharding import PartitionSpec as P

D = 4096
HEAD_DIM = 64
TAPS = 4
SSM_WIDTH = 2048
LANES = 128
SPARE = 8
KV = ("kh", "kl")
TEAM = ("kl", "tp")

EPS = 1e-06
BF16 = jnp.bfloat16
F32 = jnp.float32


def two_words(x):
    high = lax.reduce_precision(x, 8, 7)
    return high.astype(BF16), (x - high).astype(BF16)


def to_everyone(shard, axes):
    size = lax.axis_size(axes)
    return lax.all_to_all(
        jnp.broadcast_to(shard[None], (size, *shard.shape)), axes, 0, 0, tiled=True
    )


def swapped(array, dim, here, axis):
    half = array.shape[dim] // 2
    size = lax.axis_size(axis)
    mine = lax.dynamic_slice_in_dim(array, here * half, half, dim)
    other = lax.dynamic_slice_in_dim(array, (1 - here) * half, half, dim)
    return mine, lax.ppermute(other, axis, [(i, (i + 1) % size) for i in range(size)])


def in_order(mine, other, here, dim):
    return jnp.where(
        here == 0,
        jnp.concatenate([mine, other], axis=dim),
        jnp.concatenate([other, mine], axis=dim),
    )


def contract_last(a, b):
    return lax.dot_general(a, b, (((1,), (1,)), ((), ())), preferred_element_type=F32)


def project_body(x_ref, gain_ref, gate_ref, input_ref, b_ref, c_ref, step_ref, out_ref):
    stream = x_ref[...].astype(F32)
    scaled = (stream * gain_ref[...]).astype(BF16)
    dests, each = out_ref.shape[:2]
    at = 0

    def put(block):
        for k in range(dests):
            out_ref[k, :, at : at + block.shape[1]] = block[k * each : (k + 1) * each].astype(BF16)

    step = contract_last(scaled, step_ref[...])
    step_high = step.astype(BF16)
    step_low = (step - step_high.astype(F32)).astype(BF16)
    heads = step.shape[1]
    row = lax.broadcasted_iota(jnp.int32, (heads, LANES), 0)
    lane = lax.broadcasted_iota(jnp.int32, (heads, LANES), 1)
    tail = jnp.dot(step_high, (lane == row).astype(BF16), preferred_element_type=F32)
    tail += jnp.dot(step_low, (lane == row + heads).astype(BF16), preferred_element_type=F32)
    squares = jnp.sum(stream * stream, axis=1, keepdims=True)
    high = squares.astype(BF16).astype(F32)
    lane = lax.broadcasted_iota(jnp.int32, tail.shape, 1)
    tail += jnp.where(lane == 2 * heads, high, 0.0)
    tail += jnp.where(lane == 2 * heads + 1, squares - high, 0.0)
    for ref in (gate_ref, input_ref, b_ref, c_ref):
        put(jnp.dot(scaled, ref[...], preferred_element_type=F32))
        at += ref.shape[1]
    put(tail)


def project(inputs, gain_in, matrices, w_step, dests):
    rows = inputs.shape[0]
    width = sum(w.shape[1] for w in matrices) + LANES
    return pl.pallas_call(
        project_body,
        out_shape=jax.ShapeDtypeStruct((dests, rows // dests, width), BF16),
    )(inputs, gain_in[None], *matrices, w_step.T)


def prepare_body(steps_ref, lengths_ref, log_ref, state_ref, *refs):
    faded_ref, all_ref, high_ref, low_ref = refs[-4:]
    seqs, heads, block = steps_ref.shape
    rate = -jnp.exp(log_ref[...])
    position = lax.broadcasted_iota(jnp.int32, (heads, block), 1)
    after = lax.broadcasted_iota(jnp.int32, (block, block), 0) > lax.broadcasted_iota(
        jnp.int32, (block, block), 1
    )
    for b in range(seqs):
        masked = jnp.where(position < lengths_ref[b], steps_ref[b], 0.0)
        later = jnp.dot(
            masked, after.astype(F32), precision=lax.Precision.HIGHEST, preferred_element_type=F32
        )
        faded_ref[b] = jnp.exp(rate * later) * masked
        total = jnp.sum(masked, axis=1, keepdims=True)
        all_ref[b] = jnp.broadcast_to(jnp.exp(rate * total), (heads, block))
        high = state_ref[b].astype(BF16)
        high_ref[b] = high
        low_ref[b] = (state_ref[b] - high.astype(F32)).astype(BF16)


def prepare(block_step, lengths, log_column, state, others):
    steps = jnp.swapaxes(block_step, 1, 2)
    flat = state.reshape(state.shape[0], -1, state.shape[3])
    shape = pltpu.VMEM
    whole = pl.BlockSpec(memory_space=pltpu.VMEM)
    return pl.pallas_call(
        prepare_body,
        in_specs=[whole, pl.BlockSpec(memory_space=pltpu.SMEM)] + [whole] * (2 + len(others)),
        out_shape=(
            shape(steps.shape, F32),
            shape(steps.shape, F32),
            shape(flat.shape, BF16),
            shape(flat.shape, BF16),
        ),
    )(steps, lengths, log_column, flat, *others)


def on_chip(x):
    return pltpu.with_memory_space_constraint(x, pltpu.VMEM)


def silu(v):
    return v / (1.0 + jnp.exp(-v))


def mix_body(
    arrived_ref,
    conv_input_ref,
    conv_b_ref,
    conv_c_ref,
    tail_input_ref,
    tail_b_ref,
    tail_c_ref,
    bias_ref,
    log_ref,
    faded_ref,
    all_ref,
    high_ref,
    low_ref,
    values_ref,
    keys_ref,
    gain_ref,
    out_ref,
):
    seqs, heads = faded_ref.shape[:2]
    channels = gain_ref.shape[1]
    states = conv_c_ref.shape[1]
    n_state = high_ref.shape[2]
    per_group = heads * n_state // states
    total = jnp.sum(arrived_ref[...].astype(F32), axis=0)
    tail = total[:, 2 * channels + 2 * states :]
    lane = lax.broadcasted_iota(jnp.int32, tail.shape, 1)
    is_square = (lane == 2 * heads) | (lane == 2 * heads + 1)
    squares = jnp.sum(jnp.where(is_square, tail, 0.0), axis=1, keepdims=True)
    inverse = lax.rsqrt(squares / D + EPS)
    steps = (tail + pltpu.roll(tail, tail.shape[1] - heads, 1)) * inverse
    gate = silu(total[:, :channels] * inverse)

    def convolved(at, weights, history):
        summed = weights[TAPS - 1 :] * (total[:, at : at + weights.shape[1]] * inverse)
        for k in range(TAPS - 1):
            summed = summed + weights[k : k + 1] * history[k].astype(F32)
        return silu(summed)

    current = convolved(channels, conv_input_ref, tail_input_ref)
    b_now = convolved(2 * channels, conv_b_ref, tail_b_ref)
    c_now = convolved(2 * channels + states, conv_c_ref, tail_c_ref)

    rate = -jnp.exp(log_ref[...])
    head = lax.broadcasted_iota(jnp.int32, (heads, LANES), 0)
    column = lax.broadcasted_iota(jnp.int32, (heads, LANES), 1)
    key_head = lax.broadcasted_iota(jnp.int32, (heads, states), 0)
    key_lane = lax.broadcasted_iota(jnp.int32, (heads, states), 1)
    own_keys = key_lane // n_state == key_head // per_group
    out_head = lax.broadcasted_iota(jnp.int32, (heads, channels), 0)
    out_lane = lax.broadcasted_iota(jnp.int32, (heads, channels), 1)
    own_lanes = out_lane // HEAD_DIM == out_head
    head_state = lax.broadcasted_iota(jnp.int32, (heads, n_state), 0)

    def by_head(row):
        out = jnp.zeros((heads, n_state), F32)
        for g in range(states // n_state):
            part = row[:, g * n_state : (g + 1) * n_state]
            out = jnp.where(head_state // per_group == g, part, out)
        return out

    rows = []
    for b in range(seqs):
        one = slice(b, b + 1)
        step = jnp.sum(jnp.where(column == head, steps[one], 0.0), axis=1, keepdims=True)
        step = step + bias_ref[...]
        step = jnp.maximum(step, 0.0) + jnp.log1p(jnp.exp(-jnp.abs(step)))
        fade = jnp.exp(rate * step)
        query = jnp.where(own_keys, c_now[one], 0.0).astype(BF16)
        scores = contract_last(query, keys_ref[b])
        weights = (faded_ref[b] * fade * scores).astype(BF16)
        mixed = jnp.dot(weights, values_ref[b], preferred_element_type=F32)
        c_heads = by_head(c_now[one])
        c_high = c_heads.astype(BF16)
        c_low = (c_heads - c_high.astype(F32)).astype(BF16)
        readout = contract_last(c_high, high_ref[b])
        readout = readout + contract_last(c_low, high_ref[b])
        readout = readout + contract_last(c_high, low_ref[b])
        own = step * jnp.sum(c_heads * by_head(b_now[one]), axis=1, keepdims=True)
        carried = fade * all_ref[b][:, :1]
        mixed = mixed + carried * readout + own * current[one]
        rows.append(jnp.sum(jnp.where(own_lanes, mixed, 0.0), axis=0, keepdims=True))
    mixed = jnp.concatenate(rows, axis=0) * gate
    squares = jnp.sum(mixed * mixed, axis=1, keepdims=True)
    high = squares.astype(BF16).astype(F32)
    words = jnp.where(lane == 0, high, jnp.where(lane == 1, squares - high, 0.0))
    row = jnp.concatenate([mixed * gain_ref[...], words], axis=1).astype(BF16)
    for k in range(out_ref.shape[0]):
        out_ref[k] = row


def mix(arrived, convs, tails, columns, prepared, values, keys, gain, copies):
    operands = (on_chip(arrived), *convs, *tails, *columns, *[on_chip(x) for x in prepared])
    operands += (values, keys, gain)
    width = gain.shape[1] + LANES
    return pl.pallas_call(
        mix_body,
        out_shape=jax.ShapeDtypeStruct((copies, values.shape[0], width), BF16),
    )(*operands)


def lower_body(units_ref, weight_ref, out_ref):
    tiles, height, seqs = units_ref.shape
    rows = out_ref.shape[1]
    team = weight_ref.shape[2] // LANES
    lowered = jnp.zeros((seqs, weight_ref.shape[2]), F32)
    squares = jnp.zeros((seqs, LANES), F32)
    row = lax.broadcasted_iota(jnp.int32, (SPARE, LANES), 0)
    both = (row < 2).astype(BF16)
    for k in range(tiles):
        tile = units_ref[k].T
        lowered = lowered + jnp.dot(
            tile[:, : height - SPARE], weight_ref[k], preferred_element_type=F32
        )
        squares = squares + jnp.dot(
            tile[:, height - SPARE :], both, preferred_element_type=F32
        )
    scale = 1.0 / (squares / D + EPS)
    for m in range(team):
        block = (lowered[:, m * LANES : (m + 1) * LANES] * scale).astype(BF16)
        for d in range(seqs // rows):
            out_ref[d * team + m] = block[d * rows : (d + 1) * rows]


def lower(units, weight, rows):
    dests = units.shape[2] // rows * (weight.shape[2] // LANES)
    return pl.pallas_call(
        lower_body, out_shape=pltpu.VMEM((dests, rows, LANES), BF16)
    )(on_chip(units), on_chip(weight))


def layer(
    inputs,
    gain_in,
    w_gate,
    w_input,
    w_bproj,
    w_cproj,
    w_step,
    conv_input,
    conv_bproj,
    conv_cproj,
    tail_input,
    tail_bproj,
    tail_cproj,
    step_bias,
    decay_log,
    block_input,
    block_bproj,
    block_step,
    lengths,
    state,
    gain_mix,
    w_out,
    gain_mlp,
    w_up,
    w_down,
):
    core = lax.axis_index("tp")
    side = lax.axis_index("kl")
    n_kv, n_dp, n_tp = lax.axis_size(KV), lax.axis_size("dp"), lax.axis_size("tp")
    n_far, n_team = lax.axis_size("kh"), lax.axis_size(TEAM)
    rows = inputs.shape[0]
    sent = project(inputs, gain_in, (w_gate, w_input, w_bproj, w_cproj), w_step, n_kv)
    arrived = lax.all_to_all(sent, KV, 0, 0, tiled=True)
    convs = [on_chip(x) for x in (conv_input, conv_bproj, conv_cproj)]
    tails = [on_chip(jnp.swapaxes(x, 0, 1)) for x in (tail_input, tail_bproj, tail_cproj)]
    columns = [on_chip(x[:, None]) for x in (step_bias, decay_log)]
    values, keys, gain = [on_chip(x) for x in (block_input, block_bproj, gain_mix[None])]
    others = (*convs, *tails, columns[0], values, keys, gain)
    prepared = prepare(block_step, lengths, columns[1], state, others)
    scaled_up = (w_up.astype(F32) * gain_mlp[:, None]).astype(BF16)
    up_mine, up_other = swapped(scaled_up, 1, core, "tp")
    up_half = in_order(up_mine, up_other, core, 0)
    arrived, up_half = lax.optimization_barrier((arrived, up_half))
    whole = mix(arrived, convs, tails, columns, prepared, values, keys, gain, n_kv * n_tp)
    width = gain_mix.shape[0]
    whole = lax.all_to_all(whole, (*KV, "tp"), 0, 0, tiled=True)

    out_mine, out_other = swapped(w_out, 1, core, "tp")
    up_mine, up_other = swapped(up_half, 1, side, "kl")
    up_weight = in_order(up_mine, up_other, side, 0)
    down_half = in_order(*swapped(w_down, 0, core, "tp"), core, 1)
    column_count = out_mine.shape[1]
    residual = lax.dynamic_slice_in_dim(inputs, core * column_count, column_count, 1)
    whole, out_mine, out_other, up_weight, down_half, residual = lax.optimization_barrier(
        (whole, out_mine, out_other, up_weight, down_half, residual)
    )
    out_weight = jnp.concatenate([out_mine, out_other], axis=0)

    whole = whole.reshape(n_kv, n_tp, rows // n_kv, -1)
    whole = jnp.moveaxis(whole, 1, 0).reshape(n_tp, rows, -1)
    total_sq = jnp.sum(whole[:, :, width : width + 2].astype(F32), axis=(0, 2))
    halves = whole[:, :, :width]
    channels = jnp.concatenate(
        [
            lax.dynamic_index_in_dim(halves, core, 0, keepdims=False),
            lax.dynamic_index_in_dim(halves, 1 - core, 0, keepdims=False),
        ],
        axis=1,
    )
    mixed_in = jnp.dot(channels, out_weight, preferred_element_type=F32)
    mixed_in = mixed_in * lax.rsqrt(total_sq / SSM_WIDTH + EPS)[:, None]
    hidden = (residual.astype(F32) + mixed_in).astype(BF16)

    all_hidden = to_everyone(hidden, ("dp", *TEAM))
    down_weight = in_order(*swapped(down_half, 0, side, "kl"), side, 1)
    down_weight = down_weight.reshape(n_far, -1, down_weight.shape[1])
    all_hidden, down_weight = lax.optimization_barrier((all_hidden, down_weight))
    all_hidden = all_hidden.reshape(n_dp, n_team, rows, -1)
    seqs = n_dp * rows
    all_hidden = jnp.moveaxis(all_hidden, 1, 2).reshape(seqs, -1)
    raised = lax.dot_general(
        up_weight, all_hidden, (((0,), (1,)), ((), ())), preferred_element_type=F32
    ).astype(BF16)
    row_sq = jnp.sum(jnp.square(all_hidden.astype(F32)), axis=1)
    arrived = lax.all_to_all(raised.reshape(n_far, -1, seqs), "kh", 0, 0, tiled=True)
    words = jnp.concatenate(
        [*[w[None] for w in two_words(row_sq)], jnp.zeros((SPARE - 2, seqs), BF16)], axis=0
    )
    arrived, words = lax.optimization_barrier((arrived, words))
    shares = jnp.sum(arrived.astype(F32), axis=0)
    units = jnp.square(jax.nn.relu(shares)).astype(BF16)
    hidden_units = to_everyone(jnp.concatenate([units, words], axis=0), "kh")
    lowered = lower(hidden_units, down_weight, rows)
    lowered = lax.all_to_all(lowered, ("dp", *TEAM), 0, 0, tiled=True)
    return (hidden.astype(F32) + jnp.sum(lowered.astype(F32), axis=0)).astype(BF16)


def solution(mesh):
    sizes = [mesh.shape[name] for name in ("grp", "dp", "kv", "tp")]
    pairs = mesh.devices.reshape(sizes[0], sizes[1], sizes[2] // 2, 2, sizes[3])
    mesh = Mesh(pairs, ("grp", "dp", "kh", "kl", "tp"))
    return jax.shard_map(
        layer,
        mesh=mesh,
        in_specs=(
            P(("grp", "dp"), KV),
            P(KV),
            P(KV, "tp"),
            P(KV, "tp"),
            P(KV, "tp"),
            P(KV, "tp"),
            P(KV, "tp"),
            P(None, "tp"),
            P(None, "tp"),
            P(None, "tp"),
            P(("grp", "dp", *KV), None, "tp"),
            P(("grp", "dp", *KV), None, "tp"),
            P(("grp", "dp", *KV), None, "tp"),
            P("tp"),
            P("tp"),
            P(("grp", "dp", *KV), None, "tp"),
            P(("grp", "dp", *KV), None, "tp"),
            P(("grp", "dp", *KV), None, "tp"),
            P(("grp", "dp", *KV)),
            P(("grp", "dp", *KV), "tp", None, None),
            P("tp"),
            P("tp", KV),
            P((*KV, "tp")),
            P((*KV, "tp"), "dp"),
            P("dp", (*KV, "tp")),
        ),
        out_specs=P(("grp", "dp"), (*KV, "tp")),
        check_vma=False,
    )
```

```python
import jax
import jax.numpy as jnp
from jax import lax
from jax.experimental import pallas as pl
from jax.experimental.pallas import tpu as pltpu
from jax.sharding import Mesh
from jax.sharding import PartitionSpec as P

D = 4096
HEAD_DIM = 64
TAPS = 4
SSM_WIDTH = 2048
LANES = 128
SPARE = 8
KV = ("kh", "kl")
TEAM = ("kl", "tp")

EPS = 1e-06
BF16 = jnp.bfloat16
F32 = jnp.float32


def two_words(x):
    high = lax.reduce_precision(x, 8, 7)
    return high.astype(BF16), (x - high).astype(BF16)


def to_everyone(shard, axes):
    size = lax.axis_size(axes)
    return lax.all_to_all(
        jnp.broadcast_to(shard[None], (size, *shard.shape)), axes, 0, 0, tiled=True
    )


def swapped(array, dim, here, axis):
    half = array.shape[dim] // 2
    size = lax.axis_size(axis)
    mine = lax.dynamic_slice_in_dim(array, here * half, half, dim)
    other = lax.dynamic_slice_in_dim(array, (1 - here) * half, half, dim)
    return mine, lax.ppermute(other, axis, [(i, (i + 1) % size) for i in range(size)])


def in_order(mine, other, here, dim):
    return jnp.where(
        here == 0,
        jnp.concatenate([mine, other], axis=dim),
        jnp.concatenate([other, mine], axis=dim),
    )


def contract_last(a, b):
    return lax.dot_general(a, b, (((1,), (1,)), ((), ())), preferred_element_type=F32)


def project_body(x_ref, gain_ref, gate_ref, input_ref, b_ref, c_ref, step_ref, out_ref):
    stream = x_ref[...].astype(F32)
    scaled = (stream * gain_ref[...]).astype(BF16)
    dests, each = out_ref.shape[:2]
    at = 0

    def put(block):
        for k in range(dests):
            out_ref[k, :, at : at + block.shape[1]] = block[k * each : (k + 1) * each].astype(BF16)

    step = contract_last(scaled, step_ref[...])
    step_high = step.astype(BF16)
    step_low = (step - step_high.astype(F32)).astype(BF16)
    heads = step.shape[1]
    row = lax.broadcasted_iota(jnp.int32, (heads, LANES), 0)
    lane = lax.broadcasted_iota(jnp.int32, (heads, LANES), 1)
    tail = jnp.dot(step_high, (lane == row).astype(BF16), preferred_element_type=F32)
    tail += jnp.dot(step_low, (lane == row + heads).astype(BF16), preferred_element_type=F32)
    squares = jnp.sum(stream * stream, axis=1, keepdims=True)
    high = squares.astype(BF16).astype(F32)
    lane = lax.broadcasted_iota(jnp.int32, tail.shape, 1)
    tail += jnp.where(lane == 2 * heads, high, 0.0)
    tail += jnp.where(lane == 2 * heads + 1, squares - high, 0.0)
    for ref in (gate_ref, input_ref, b_ref, c_ref):
        put(jnp.dot(scaled, ref[...], preferred_element_type=F32))
        at += ref.shape[1]
    put(tail)


def project(inputs, gain_in, matrices, w_step, dests):
    rows = inputs.shape[0]
    width = sum(w.shape[1] for w in matrices) + LANES
    return pl.pallas_call(
        project_body,
        out_shape=jax.ShapeDtypeStruct((dests, rows // dests, width), BF16),
    )(inputs, gain_in[None], *matrices, w_step.T)


def prepare_body(steps_ref, lengths_ref, log_ref, state_ref, *refs):
    faded_ref, all_ref, high_ref, low_ref = refs[-4:]
    seqs, heads, block = steps_ref.shape
    rate = -jnp.exp(log_ref[...])
    position = lax.broadcasted_iota(jnp.int32, (heads, block), 1)
    after = lax.broadcasted_iota(jnp.int32, (block, block), 0) > lax.broadcasted_iota(
        jnp.int32, (block, block), 1
    )
    for b in range(seqs):
        masked = jnp.where(position < lengths_ref[b], steps_ref[b], 0.0)
        later = jnp.dot(
            masked, after.astype(F32), precision=lax.Precision.HIGHEST, preferred_element_type=F32
        )
        faded_ref[b] = jnp.exp(rate * later) * masked
        total = jnp.sum(masked, axis=1, keepdims=True)
        all_ref[b] = jnp.broadcast_to(jnp.exp(rate * total), (heads, block))
        high = state_ref[b].astype(BF16)
        high_ref[b] = high
        low_ref[b] = (state_ref[b] - high.astype(F32)).astype(BF16)


def prepare(block_step, lengths, log_column, state, others):
    steps = jnp.swapaxes(block_step, 1, 2)
    flat = state.reshape(state.shape[0], -1, state.shape[3])
    shape = pltpu.VMEM
    whole = pl.BlockSpec(memory_space=pltpu.VMEM)
    return pl.pallas_call(
        prepare_body,
        in_specs=[whole, pl.BlockSpec(memory_space=pltpu.SMEM)] + [whole] * (2 + len(others)),
        out_shape=(
            shape(steps.shape, F32),
            shape(steps.shape, F32),
            shape(flat.shape, BF16),
            shape(flat.shape, BF16),
        ),
    )(steps, lengths, log_column, flat, *others)


def on_chip(x):
    return pltpu.with_memory_space_constraint(x, pltpu.VMEM)


def silu(v):
    return v / (1.0 + jnp.exp(-v))


def mix_body(
    arrived_ref,
    conv_input_ref,
    conv_b_ref,
    conv_c_ref,
    tail_input_ref,
    tail_b_ref,
    tail_c_ref,
    bias_ref,
    log_ref,
    faded_ref,
    all_ref,
    high_ref,
    low_ref,
    values_ref,
    keys_ref,
    gain_ref,
    out_ref,
):
    seqs, heads = faded_ref.shape[:2]
    channels = gain_ref.shape[1]
    states = conv_c_ref.shape[1]
    n_state = high_ref.shape[2]
    per_group = heads * n_state // states
    total = jnp.sum(arrived_ref[...].astype(F32), axis=0)
    tail = total[:, 2 * channels + 2 * states :]
    lane = lax.broadcasted_iota(jnp.int32, tail.shape, 1)
    is_square = (lane == 2 * heads) | (lane == 2 * heads + 1)
    squares = jnp.sum(jnp.where(is_square, tail, 0.0), axis=1, keepdims=True)
    inverse = lax.rsqrt(squares / D + EPS)
    steps = (tail + pltpu.roll(tail, tail.shape[1] - heads, 1)) * inverse
    gate = silu(total[:, :channels] * inverse)

    def convolved(at, weights, history):
        summed = weights[TAPS - 1 :] * (total[:, at : at + weights.shape[1]] * inverse)
        for k in range(TAPS - 1):
            summed = summed + weights[k : k + 1] * history[k].astype(F32)
        return silu(summed)

    current = convolved(channels, conv_input_ref, tail_input_ref)
    b_now = convolved(2 * channels, conv_b_ref, tail_b_ref)
    c_now = convolved(2 * channels + states, conv_c_ref, tail_c_ref)

    rate = -jnp.exp(log_ref[...])
    head = lax.broadcasted_iota(jnp.int32, (heads, LANES), 0)
    column = lax.broadcasted_iota(jnp.int32, (heads, LANES), 1)
    key_head = lax.broadcasted_iota(jnp.int32, (heads, states), 0)
    key_lane = lax.broadcasted_iota(jnp.int32, (heads, states), 1)
    own_keys = key_lane // n_state == key_head // per_group
    out_head = lax.broadcasted_iota(jnp.int32, (heads, channels), 0)
    out_lane = lax.broadcasted_iota(jnp.int32, (heads, channels), 1)
    own_lanes = out_lane // HEAD_DIM == out_head
    head_state = lax.broadcasted_iota(jnp.int32, (heads, n_state), 0)

    def by_head(row):
        out = jnp.zeros((heads, n_state), F32)
        for g in range(states // n_state):
            part = row[:, g * n_state : (g + 1) * n_state]
            out = jnp.where(head_state // per_group == g, part, out)
        return out

    rows = []
    for b in range(seqs):
        one = slice(b, b + 1)
        step = jnp.sum(jnp.where(column == head, steps[one], 0.0), axis=1, keepdims=True)
        step = step + bias_ref[...]
        step = jnp.maximum(step, 0.0) + jnp.log1p(jnp.exp(-jnp.abs(step)))
        fade = jnp.exp(rate * step)
        query = jnp.where(own_keys, c_now[one], 0.0).astype(BF16)
        scores = contract_last(query, keys_ref[b])
        weights = (faded_ref[b] * fade * scores).astype(BF16)
        mixed = jnp.dot(weights, values_ref[b], preferred_element_type=F32)
        c_heads = by_head(c_now[one])
        c_high = c_heads.astype(BF16)
        c_low = (c_heads - c_high.astype(F32)).astype(BF16)
        readout = contract_last(c_high, high_ref[b])
        readout = readout + contract_last(c_low, high_ref[b])
        readout = readout + contract_last(c_high, low_ref[b])
        own = step * jnp.sum(c_heads * by_head(b_now[one]), axis=1, keepdims=True)
        carried = fade * all_ref[b][:, :1]
        mixed = mixed + carried * readout + own * current[one]
        rows.append(jnp.sum(jnp.where(own_lanes, mixed, 0.0), axis=0, keepdims=True))
    mixed = jnp.concatenate(rows, axis=0) * gate
    squares = jnp.sum(mixed * mixed, axis=1, keepdims=True)
    high = squares.astype(BF16).astype(F32)
    words = jnp.where(lane == 0, high, jnp.where(lane == 1, squares - high, 0.0))
    row = jnp.concatenate([mixed * gain_ref[...], words], axis=1).astype(BF16)
    for k in range(out_ref.shape[0]):
        out_ref[k] = row


def mix(arrived, convs, tails, columns, prepared, values, keys, gain, copies):
    operands = (on_chip(arrived), *convs, *tails, *columns, *[on_chip(x) for x in prepared])
    operands += (values, keys, gain)
    width = gain.shape[1] + LANES
    return pl.pallas_call(
        mix_body,
        out_shape=jax.ShapeDtypeStruct((copies, values.shape[0], width), BF16),
    )(*operands)


def lower_body(units_ref, weight_ref, out_ref):
    tiles, height, seqs = units_ref.shape
    rows = out_ref.shape[1]
    team = weight_ref.shape[2] // LANES
    lowered = jnp.zeros((seqs, weight_ref.shape[2]), F32)
    squares = jnp.zeros((seqs, LANES), F32)
    row = lax.broadcasted_iota(jnp.int32, (SPARE, LANES), 0)
    both = (row < 2).astype(BF16)
    for k in range(tiles):
        tile = units_ref[k].T
        lowered = lowered + jnp.dot(
            tile[:, : height - SPARE], weight_ref[k], preferred_element_type=F32
        )
        squares = squares + jnp.dot(
            tile[:, height - SPARE :], both, preferred_element_type=F32
        )
    scale = 1.0 / (squares / D + EPS)
    for m in range(team):
        block = (lowered[:, m * LANES : (m + 1) * LANES] * scale).astype(BF16)
        for d in range(seqs // rows):
            out_ref[d * team + m] = block[d * rows : (d + 1) * rows]


def lower(units, weight, rows):
    dests = units.shape[2] // rows * (weight.shape[2] // LANES)
    return pl.pallas_call(
        lower_body, out_shape=pltpu.VMEM((dests, rows, LANES), BF16)
    )(on_chip(units), on_chip(weight))


def layer(
    inputs,
    gain_in,
    w_gate,
    w_input,
    w_bproj,
    w_cproj,
    w_step,
    conv_input,
    conv_bproj,
    conv_cproj,
    tail_input,
    tail_bproj,
    tail_cproj,
    step_bias,
    decay_log,
    block_input,
    block_bproj,
    block_step,
    lengths,
    state,
    gain_mix,
    w_out,
    gain_mlp,
    w_up,
    w_down,
):
    core = lax.axis_index("tp")
    side = lax.axis_index("kl")
    n_kv, n_dp, n_tp = lax.axis_size(KV), lax.axis_size("dp"), lax.axis_size("tp")
    n_far, n_team = lax.axis_size("kh"), lax.axis_size(TEAM)
    rows = inputs.shape[0]
    sent = project(inputs, gain_in, (w_gate, w_input, w_bproj, w_cproj), w_step, n_kv)
    arrived = lax.all_to_all(sent, KV, 0, 0, tiled=True)
    convs = [on_chip(x) for x in (conv_input, conv_bproj, conv_cproj)]
    tails = [on_chip(jnp.swapaxes(x, 0, 1)) for x in (tail_input, tail_bproj, tail_cproj)]
    columns = [on_chip(x[:, None]) for x in (step_bias, decay_log)]
    values, keys, gain = [on_chip(x) for x in (block_input, block_bproj, gain_mix[None])]
    others = (*convs, *tails, columns[0], values, keys, gain)
    prepared = prepare(block_step, lengths, columns[1], state, others)
    scaled_up = (w_up.astype(F32) * gain_mlp[:, None]).astype(BF16)
    up_mine, up_other = swapped(scaled_up, 1, core, "tp")
    up_half = in_order(up_mine, up_other, core, 0)
    arrived, up_half = lax.optimization_barrier((arrived, up_half))
    whole = mix(arrived, convs, tails, columns, prepared, values, keys, gain, n_kv * n_tp)
    width = gain_mix.shape[0]
    whole = lax.all_to_all(whole, (*KV, "tp"), 0, 0, tiled=True)

    out_mine, out_other = swapped(w_out, 1, core, "tp")
    up_mine, up_other = swapped(up_half, 1, side, "kl")
    up_weight = in_order(up_mine, up_other, side, 0)
    down_half = in_order(*swapped(w_down, 0, core, "tp"), core, 1)
    column_count = out_mine.shape[1]
    residual = lax.dynamic_slice_in_dim(inputs, core * column_count, column_count, 1)
    whole, out_mine, out_other, residual = lax.optimization_barrier(
        (whole, out_mine, out_other, residual)
    )
    out_weight = jnp.concatenate([out_mine, out_other], axis=0)

    whole = whole.reshape(n_kv, n_tp, rows // n_kv, -1)
    whole = jnp.moveaxis(whole, 1, 0).reshape(n_tp, rows, -1)
    total_sq = jnp.sum(whole[:, :, width : width + 2].astype(F32), axis=(0, 2))
    halves = whole[:, :, :width]
    channels = jnp.concatenate(
        [
            lax.dynamic_index_in_dim(halves, core, 0, keepdims=False),
            lax.dynamic_index_in_dim(halves, 1 - core, 0, keepdims=False),
        ],
        axis=1,
    )
    mixed_in = jnp.dot(channels, out_weight, preferred_element_type=F32)
    mixed_in = mixed_in * lax.rsqrt(total_sq / SSM_WIDTH + EPS)[:, None]
    hidden = (residual.astype(F32) + mixed_in).astype(BF16)

    all_hidden = to_everyone(hidden, ("dp", *TEAM))
    down_weight = in_order(*swapped(down_half, 0, side, "kl"), side, 1)
    down_weight = down_weight.reshape(n_far, -1, down_weight.shape[1])
    all_hidden, up_weight = lax.optimization_barrier((all_hidden, up_weight))
    all_hidden = all_hidden.reshape(n_dp, n_team, rows, -1)
    seqs = n_dp * rows
    all_hidden = jnp.moveaxis(all_hidden, 1, 2).reshape(seqs, -1)
    raised = lax.dot_general(
        up_weight, all_hidden, (((0,), (1,)), ((), ())), preferred_element_type=F32
    ).astype(BF16)
    row_sq = jnp.sum(jnp.square(all_hidden.astype(F32)), axis=1)
    arrived = lax.all_to_all(raised.reshape(n_far, -1, seqs), "kh", 0, 0, tiled=True)
    words = jnp.concatenate(
        [*[w[None] for w in two_words(row_sq)], jnp.zeros((SPARE - 2, seqs), BF16)], axis=0
    )
    arrived, words, down_weight = lax.optimization_barrier((arrived, words, down_weight))
    shares = jnp.sum(arrived.astype(F32), axis=0)
    units = jnp.square(jax.nn.relu(shares)).astype(BF16)
    hidden_units = to_everyone(jnp.concatenate([units, words], axis=0), "kh")
    lowered = lower(hidden_units, down_weight, rows)
    lowered = lax.all_to_all(lowered, ("dp", *TEAM), 0, 0, tiled=True)
    return (hidden.astype(F32) + jnp.sum(lowered.astype(F32), axis=0)).astype(BF16)


def solution(mesh):
    sizes = [mesh.shape[name] for name in ("grp", "dp", "kv", "tp")]
    pairs = mesh.devices.reshape(sizes[0], sizes[1], sizes[2] // 2, 2, sizes[3])
    mesh = Mesh(pairs, ("grp", "dp", "kh", "kl", "tp"))
    return jax.shard_map(
        layer,
        mesh=mesh,
        in_specs=(
            P(("grp", "dp"), KV),
            P(KV),
            P(KV, "tp"),
            P(KV, "tp"),
            P(KV, "tp"),
            P(KV, "tp"),
            P(KV, "tp"),
            P(None, "tp"),
            P(None, "tp"),
            P(None, "tp"),
            P(("grp", "dp", *KV), None, "tp"),
            P(("grp", "dp", *KV), None, "tp"),
            P(("grp", "dp", *KV), None, "tp"),
            P("tp"),
            P("tp"),
            P(("grp", "dp", *KV), None, "tp"),
            P(("grp", "dp", *KV), None, "tp"),
            P(("grp", "dp", *KV), None, "tp"),
            P(("grp", "dp", *KV)),
            P(("grp", "dp", *KV), "tp", None, None),
            P("tp"),
            P("tp", KV),
            P((*KV, "tp")),
            P((*KV, "tp"), "dp"),
            P("dp", (*KV, "tp")),
        ),
        out_specs=P(("grp", "dp"), (*KV, "tp")),
        check_vma=False,
    )
```

```python
import jax
import jax.numpy as jnp
from jax import lax
from jax.experimental import pallas as pl
from jax.experimental.pallas import tpu as pltpu
from jax.sharding import Mesh
from jax.sharding import PartitionSpec as P

D = 4096
HEAD_DIM = 64
TAPS = 4
SSM_WIDTH = 2048
LANES = 128
SPARE = 8
KV = ("kh", "kl")
TEAM = ("kl", "tp")

EPS = 1e-06
BF16 = jnp.bfloat16
F32 = jnp.float32


def two_words(x):
    high = lax.reduce_precision(x, 8, 7)
    return high.astype(BF16), (x - high).astype(BF16)


def to_everyone(shard, axes):
    size = lax.axis_size(axes)
    return lax.all_to_all(
        jnp.broadcast_to(shard[None], (size, *shard.shape)), axes, 0, 0, tiled=True
    )


def swapped(array, dim, here, axis):
    half = array.shape[dim] // 2
    size = lax.axis_size(axis)
    mine = lax.dynamic_slice_in_dim(array, here * half, half, dim)
    other = lax.dynamic_slice_in_dim(array, (1 - here) * half, half, dim)
    return mine, lax.ppermute(other, axis, [(i, (i + 1) % size) for i in range(size)])


def in_order(mine, other, here, dim):
    return jnp.where(
        here == 0,
        jnp.concatenate([mine, other], axis=dim),
        jnp.concatenate([other, mine], axis=dim),
    )


def contract_last(a, b):
    return lax.dot_general(a, b, (((1,), (1,)), ((), ())), preferred_element_type=F32)


def project_body(x_ref, gain_ref, gate_ref, input_ref, b_ref, c_ref, step_ref, out_ref):
    stream = x_ref[...].astype(F32)
    scaled = (stream * gain_ref[...]).astype(BF16)
    dests, each = out_ref.shape[:2]
    at = 0

    def put(block):
        for k in range(dests):
            out_ref[k, :, at : at + block.shape[1]] = block[k * each : (k + 1) * each].astype(BF16)

    step = contract_last(scaled, step_ref[...])
    step_high = step.astype(BF16)
    step_low = (step - step_high.astype(F32)).astype(BF16)
    heads = step.shape[1]
    row = lax.broadcasted_iota(jnp.int32, (heads, LANES), 0)
    lane = lax.broadcasted_iota(jnp.int32, (heads, LANES), 1)
    tail = jnp.dot(step_high, (lane == row).astype(BF16), preferred_element_type=F32)
    tail += jnp.dot(step_low, (lane == row + heads).astype(BF16), preferred_element_type=F32)
    squares = jnp.sum(stream * stream, axis=1, keepdims=True)
    high = squares.astype(BF16).astype(F32)
    lane = lax.broadcasted_iota(jnp.int32, tail.shape, 1)
    tail += jnp.where(lane == 2 * heads, high, 0.0)
    tail += jnp.where(lane == 2 * heads + 1, squares - high, 0.0)
    for ref in (gate_ref, input_ref, b_ref, c_ref):
        put(jnp.dot(scaled, ref[...], preferred_element_type=F32))
        at += ref.shape[1]
    put(tail)


def project(inputs, gain_in, matrices, w_step, dests):
    rows = inputs.shape[0]
    width = sum(w.shape[1] for w in matrices) + LANES
    return pl.pallas_call(
        project_body,
        out_shape=jax.ShapeDtypeStruct((dests, rows // dests, width), BF16),
    )(inputs, gain_in[None], *matrices, w_step.T)


def prepare_body(steps_ref, lengths_ref, log_ref, state_ref, *refs):
    faded_ref, all_ref, high_ref, low_ref = refs[-4:]
    seqs, heads, block = steps_ref.shape
    rate = -jnp.exp(log_ref[...])
    position = lax.broadcasted_iota(jnp.int32, (heads, block), 1)
    after = lax.broadcasted_iota(jnp.int32, (block, block), 0) > lax.broadcasted_iota(
        jnp.int32, (block, block), 1
    )
    for b in range(seqs):
        masked = jnp.where(position < lengths_ref[b], steps_ref[b], 0.0)
        later = jnp.dot(
            masked, after.astype(F32), precision=lax.Precision.HIGHEST, preferred_element_type=F32
        )
        faded_ref[b] = jnp.exp(rate * later) * masked
        total = jnp.sum(masked, axis=1, keepdims=True)
        all_ref[b] = jnp.broadcast_to(jnp.exp(rate * total), (heads, block))
        high = state_ref[b].astype(BF16)
        high_ref[b] = high
        low_ref[b] = (state_ref[b] - high.astype(F32)).astype(BF16)


def prepare(block_step, lengths, log_column, state, others):
    steps = jnp.swapaxes(block_step, 1, 2)
    flat = state.reshape(state.shape[0], -1, state.shape[3])
    shape = pltpu.VMEM
    whole = pl.BlockSpec(memory_space=pltpu.VMEM)
    return pl.pallas_call(
        prepare_body,
        in_specs=[whole, pl.BlockSpec(memory_space=pltpu.SMEM)] + [whole] * (2 + len(others)),
        out_shape=(
            shape(steps.shape, F32),
            shape(steps.shape, F32),
            shape(flat.shape, BF16),
            shape(flat.shape, BF16),
        ),
    )(steps, lengths, log_column, flat, *others)


def on_chip(x):
    return pltpu.with_memory_space_constraint(x, pltpu.VMEM)


def silu(v):
    return v / (1.0 + jnp.exp(-v))


def mix_body(
    arrived_ref,
    conv_input_ref,
    conv_b_ref,
    conv_c_ref,
    tail_input_ref,
    tail_b_ref,
    tail_c_ref,
    bias_ref,
    log_ref,
    faded_ref,
    all_ref,
    high_ref,
    low_ref,
    values_ref,
    keys_ref,
    gain_ref,
    out_ref,
):
    seqs, heads = faded_ref.shape[:2]
    channels = gain_ref.shape[1]
    states = conv_c_ref.shape[1]
    n_state = high_ref.shape[2]
    per_group = heads * n_state // states
    total = jnp.sum(arrived_ref[...].astype(F32), axis=0)
    tail = total[:, 2 * channels + 2 * states :]
    lane = lax.broadcasted_iota(jnp.int32, tail.shape, 1)
    is_square = (lane == 2 * heads) | (lane == 2 * heads + 1)
    squares = jnp.sum(jnp.where(is_square, tail, 0.0), axis=1, keepdims=True)
    inverse = lax.rsqrt(squares / D + EPS)
    steps = (tail + pltpu.roll(tail, tail.shape[1] - heads, 1)) * inverse
    gate = silu(total[:, :channels] * inverse)

    def convolved(at, weights, history):
        summed = weights[TAPS - 1 :] * (total[:, at : at + weights.shape[1]] * inverse)
        for k in range(TAPS - 1):
            summed = summed + weights[k : k + 1] * history[k].astype(F32)
        return silu(summed)

    current = convolved(channels, conv_input_ref, tail_input_ref)
    b_now = convolved(2 * channels, conv_b_ref, tail_b_ref)
    c_now = convolved(2 * channels + states, conv_c_ref, tail_c_ref)

    rate = -jnp.exp(log_ref[...])
    head = lax.broadcasted_iota(jnp.int32, (heads, LANES), 0)
    column = lax.broadcasted_iota(jnp.int32, (heads, LANES), 1)
    key_head = lax.broadcasted_iota(jnp.int32, (heads, states), 0)
    key_lane = lax.broadcasted_iota(jnp.int32, (heads, states), 1)
    own_keys = key_lane // n_state == key_head // per_group
    out_head = lax.broadcasted_iota(jnp.int32, (heads, channels), 0)
    out_lane = lax.broadcasted_iota(jnp.int32, (heads, channels), 1)
    own_lanes = out_lane // HEAD_DIM == out_head
    head_state = lax.broadcasted_iota(jnp.int32, (heads, n_state), 0)

    def by_head(row):
        out = jnp.zeros((heads, n_state), F32)
        for g in range(states // n_state):
            part = row[:, g * n_state : (g + 1) * n_state]
            out = jnp.where(head_state // per_group == g, part, out)
        return out

    rows = []
    for b in range(seqs):
        one = slice(b, b + 1)
        step = jnp.sum(jnp.where(column == head, steps[one], 0.0), axis=1, keepdims=True)
        step = step + bias_ref[...]
        step = jnp.maximum(step, 0.0) + jnp.log1p(jnp.exp(-jnp.abs(step)))
        fade = jnp.exp(rate * step)
        query = jnp.where(own_keys, c_now[one], 0.0).astype(BF16)
        scores = contract_last(query, keys_ref[b])
        weights = (faded_ref[b] * fade * scores).astype(BF16)
        mixed = jnp.dot(weights, values_ref[b], preferred_element_type=F32)
        c_heads = by_head(c_now[one])
        c_high = c_heads.astype(BF16)
        c_low = (c_heads - c_high.astype(F32)).astype(BF16)
        readout = contract_last(c_high, high_ref[b])
        readout = readout + contract_last(c_low, high_ref[b])
        readout = readout + contract_last(c_high, low_ref[b])
        own = step * jnp.sum(c_heads * by_head(b_now[one]), axis=1, keepdims=True)
        carried = fade * all_ref[b][:, :1]
        mixed = mixed + carried * readout + own * current[one]
        rows.append(jnp.sum(jnp.where(own_lanes, mixed, 0.0), axis=0, keepdims=True))
    mixed = jnp.concatenate(rows, axis=0) * gate
    squares = jnp.sum(mixed * mixed, axis=1, keepdims=True)
    high = squares.astype(BF16).astype(F32)
    words = jnp.where(lane == 0, high, jnp.where(lane == 1, squares - high, 0.0))
    row = jnp.concatenate([mixed * gain_ref[...], words], axis=1).astype(BF16)
    for k in range(out_ref.shape[0]):
        out_ref[k] = row


def mix(arrived, convs, tails, columns, prepared, values, keys, gain, copies):
    operands = (on_chip(arrived), *convs, *tails, *columns, *[on_chip(x) for x in prepared])
    operands += (values, keys, gain)
    width = gain.shape[1] + LANES
    return pl.pallas_call(
        mix_body,
        out_shape=jax.ShapeDtypeStruct((copies, values.shape[0], width), BF16),
    )(*operands)


def emit_body(core_ref, whole_ref, mine_ref, other_ref, residual_ref, out_ref, hidden_ref, half_ref):
    core = core_ref[0]
    each = whole_ref.shape[1]
    width = mine_ref.shape[0]
    for k in range(whole_ref.shape[0] // 2):
        at = slice(k * each, (k + 1) * each)
        half_ref[0, at] = whole_ref[2 * k + core].astype(F32)
        half_ref[1, at] = whole_ref[2 * k + 1 - core].astype(F32)
    own, partner = half_ref[0], half_ref[1]
    mixed = jnp.dot(own[:, :width].astype(BF16), mine_ref[...], preferred_element_type=F32)
    mixed = mixed + jnp.dot(
        partner[:, :width].astype(BF16), other_ref[...], preferred_element_type=F32
    )
    squares = jnp.sum(own[:, width:] + partner[:, width:], axis=1, keepdims=True)
    mixed = mixed * lax.rsqrt(squares / SSM_WIDTH + EPS)
    hidden = (residual_ref[...].astype(F32) + mixed).astype(BF16)
    hidden_ref[...] = hidden
    for m in range(out_ref.shape[0]):
        out_ref[m] = hidden


def emit(core, whole, mine, other, residual, copies):
    shape = residual.shape
    in_chip = pl.BlockSpec(memory_space=pltpu.VMEM)
    return pl.pallas_call(
        emit_body,
        in_specs=[pl.BlockSpec(memory_space=pltpu.SMEM)] + [in_chip] * 4,
        out_shape=(jax.ShapeDtypeStruct((copies, *shape), BF16), pltpu.VMEM(shape, BF16)),
        scratch_shapes=[pltpu.VMEM((2, shape[0], whole.shape[2]), F32)],
    )(core[None], *[on_chip(x) for x in (whole, mine, other, residual)])


def lower_body(units_ref, weight_ref, out_ref):
    tiles, height, seqs = units_ref.shape
    rows = out_ref.shape[1]
    team = weight_ref.shape[2] // LANES
    lowered = jnp.zeros((seqs, weight_ref.shape[2]), F32)
    squares = jnp.zeros((seqs, LANES), F32)
    row = lax.broadcasted_iota(jnp.int32, (SPARE, LANES), 0)
    both = (row < 2).astype(BF16)
    for k in range(tiles):
        tile = units_ref[k].T
        lowered = lowered + jnp.dot(
            tile[:, : height - SPARE], weight_ref[k], preferred_element_type=F32
        )
        squares = squares + jnp.dot(
            tile[:, height - SPARE :], both, preferred_element_type=F32
        )
    scale = 1.0 / (squares / D + EPS)
    for m in range(team):
        block = (lowered[:, m * LANES : (m + 1) * LANES] * scale).astype(BF16)
        for d in range(seqs // rows):
            out_ref[d * team + m] = block[d * rows : (d + 1) * rows]


def lower(units, weight, rows):
    dests = units.shape[2] // rows * (weight.shape[2] // LANES)
    return pl.pallas_call(
        lower_body, out_shape=pltpu.VMEM((dests, rows, LANES), BF16)
    )(on_chip(units), on_chip(weight))


def layer(
    inputs,
    gain_in,
    w_gate,
    w_input,
    w_bproj,
    w_cproj,
    w_step,
    conv_input,
    conv_bproj,
    conv_cproj,
    tail_input,
    tail_bproj,
    tail_cproj,
    step_bias,
    decay_log,
    block_input,
    block_bproj,
    block_step,
    lengths,
    state,
    gain_mix,
    w_out,
    gain_mlp,
    w_up,
    w_down,
):
    core = lax.axis_index("tp")
    side = lax.axis_index("kl")
    n_kv, n_dp, n_tp = lax.axis_size(KV), lax.axis_size("dp"), lax.axis_size("tp")
    n_far, n_team = lax.axis_size("kh"), lax.axis_size(TEAM)
    rows = inputs.shape[0]
    sent = project(inputs, gain_in, (w_gate, w_input, w_bproj, w_cproj), w_step, n_kv)
    arrived = lax.all_to_all(sent, KV, 0, 0, tiled=True)
    convs = [on_chip(x) for x in (conv_input, conv_bproj, conv_cproj)]
    tails = [on_chip(jnp.swapaxes(x, 0, 1)) for x in (tail_input, tail_bproj, tail_cproj)]
    columns = [on_chip(x[:, None]) for x in (step_bias, decay_log)]
    values, keys, gain = [on_chip(x) for x in (block_input, block_bproj, gain_mix[None])]
    others = (*convs, *tails, columns[0], values, keys, gain)
    prepared = prepare(block_step, lengths, columns[1], state, others)
    scaled_up = (w_up.astype(F32) * gain_mlp[:, None]).astype(BF16)
    up_mine, up_other = swapped(scaled_up, 1, core, "tp")
    up_half = in_order(up_mine, up_other, core, 0)
    down_half = in_order(*swapped(w_down, 0, core, "tp"), core, 1)
    arrived, up_half, down_half = lax.optimization_barrier((arrived, up_half, down_half))
    whole = mix(arrived, convs, tails, columns, prepared, values, keys, gain, n_kv * n_tp)
    whole = lax.all_to_all(whole, (*KV, "tp"), 0, 0, tiled=True)

    out_mine, out_other = swapped(w_out, 1, core, "tp")
    up_mine, up_other = swapped(up_half, 1, side, "kl")
    up_weight = in_order(up_mine, up_other, side, 0)
    column_count = out_mine.shape[1]
    residual = lax.dynamic_slice_in_dim(inputs, core * column_count, column_count, 1)
    whole, out_mine, out_other, residual = lax.optimization_barrier(
        (whole, out_mine, out_other, residual)
    )
    copies, hidden = emit(core, whole, out_mine, out_other, residual, n_dp * n_team)
    all_hidden = lax.all_to_all(copies, ("dp", *TEAM), 0, 0, tiled=True)
    down_weight = in_order(*swapped(down_half, 0, side, "kl"), side, 1)
    down_weight = down_weight.reshape(n_far, -1, down_weight.shape[1])
    all_hidden, up_weight = lax.optimization_barrier((all_hidden, up_weight))
    all_hidden = all_hidden.reshape(n_dp, n_team, rows, -1)
    seqs = n_dp * rows
    all_hidden = jnp.moveaxis(all_hidden, 1, 2).reshape(seqs, -1)
    raised = lax.dot_general(
        up_weight, all_hidden, (((0,), (1,)), ((), ())), preferred_element_type=F32
    ).astype(BF16)
    row_sq = jnp.sum(jnp.square(all_hidden.astype(F32)), axis=1)
    arrived = lax.all_to_all(raised.reshape(n_far, -1, seqs), "kh", 0, 0, tiled=True)
    words = jnp.concatenate(
        [*[w[None] for w in two_words(row_sq)], jnp.zeros((SPARE - 2, seqs), BF16)], axis=0
    )
    arrived, words, down_weight = lax.optimization_barrier((arrived, words, down_weight))
    shares = jnp.sum(arrived.astype(F32), axis=0)
    units = jnp.square(jax.nn.relu(shares)).astype(BF16)
    hidden_units = to_everyone(jnp.concatenate([units, words], axis=0), "kh")
    lowered = lower(hidden_units, down_weight, rows)
    lowered = lax.all_to_all(lowered, ("dp", *TEAM), 0, 0, tiled=True)
    return (hidden.astype(F32) + jnp.sum(lowered.astype(F32), axis=0)).astype(BF16)


def solution(mesh):
    sizes = [mesh.shape[name] for name in ("grp", "dp", "kv", "tp")]
    pairs = mesh.devices.reshape(sizes[0], sizes[1], sizes[2] // 2, 2, sizes[3])
    mesh = Mesh(pairs, ("grp", "dp", "kh", "kl", "tp"))
    return jax.shard_map(
        layer,
        mesh=mesh,
        in_specs=(
            P(("grp", "dp"), KV),
            P(KV),
            P(KV, "tp"),
            P(KV, "tp"),
            P(KV, "tp"),
            P(KV, "tp"),
            P(KV, "tp"),
            P(None, "tp"),
            P(None, "tp"),
            P(None, "tp"),
            P(("grp", "dp", *KV), None, "tp"),
            P(("grp", "dp", *KV), None, "tp"),
            P(("grp", "dp", *KV), None, "tp"),
            P("tp"),
            P("tp"),
            P(("grp", "dp", *KV), None, "tp"),
            P(("grp", "dp", *KV), None, "tp"),
            P(("grp", "dp", *KV), None, "tp"),
            P(("grp", "dp", *KV)),
            P(("grp", "dp", *KV), "tp", None, None),
            P("tp"),
            P("tp", KV),
            P((*KV, "tp")),
            P((*KV, "tp"), "dp"),
            P("dp", (*KV, "tp")),
        ),
        out_specs=P(("grp", "dp"), (*KV, "tp")),
        check_vma=False,
    )
```
